32 devices in a mesh: sp: 8 (over z, y), dp: 4 (over x, core).
Axes of the slice: x: 2, y: 2, z: 4, core: 2. Of those that a mesh axis runs over, the one named last changes fastest.
Arguments:
- u_pre: bfloat16 [4, 8192, 2048], P('dp', 'sp'), may hold values from -6 to 6
- v_pre: bfloat16 [4, 8192, 2048], P('dp', 'sp'), may hold values from -6 to 6
- d_out: bfloat16 [4, 8192, 2048], P('dp', 'sp'), may hold values from -6 to 6
- w_mix: bfloat16 [16, 128, 128], replicated, may hold values from -0.5 to 0.5
- mix_bias: float32 [16, 128], replicated, may hold values from 0.1 to 1.9
- norm_gain: float32 [16, 128], replicated, may hold values from 0.1 to 1.9
- norm_shift: float32 [16, 128], replicated, may hold values from -3 to 3
- w_out: bfloat16 [2048, 2048], P('dp'), may hold values from -0.125 to 0.125
Outputs:
- grad_u: bfloat16 [4, 8192, 2048], P('dp', 'sp')
- grad_v: bfloat16 [4, 8192, 2048], P('dp', 'sp')
- grad_w_out: float32 [2048, 2048], P('dp')
- grad_w_mix: float32 [16, 128, 128], replicated
- grad_mix_bias: float32 [16, 128], replicated
- grad_gain: float32 [16, 128], replicated
- grad_shift: float32 [16, 128], replicated
The draws below stay inside these ranges and needn't reach their ends.
All inputs are finite; a program needn't handle non-finite values.
Results may differ from the reference program's by a relative error of at most 0.012.
Values may be sent and summed in bfloat16 or wider, within the bound.
No kernel may reach another device: no remote copies, remote signals or barrier semaphores. Data moves between devices by JAX's collectives and lax.ppermute only.
A program may use at most 192 MiB of HBM per device.

```python
import jax
import jax.numpy as jnp
from jax import lax

D = 2048
GROUPS = 16
CHANS = 128
BLOCK = 128
SGU_W = 2048
SEQLEN = 8192
SEQS = 4


def block_scale(stream_key, extent, shards, least, largest):
    def one(axis_at, blocks):
        heights = jax.random.uniform(jax.random.fold_in(jax.random.fold_in(stream_key, 6), axis_at), (blocks,), jnp.float32, least / len(shards), largest / len(shards))
        return jnp.repeat(jnp.exp(heights), extent[axis_at] // blocks).reshape((-1,) + (1,) * (len(extent) - axis_at - 1))

    factor_of = one(*shards[0])
    for cut in shards[1:]:
        factor_of = factor_of * one(*cut)
    return factor_of


def scatter_about(stream_key, shape, spread, bound, split=(), kind=jnp.bfloat16):
    entries = jax.random.normal(stream_key, shape, jnp.float32) * spread
    if len(split) > 0:
        entries = block_scale(stream_key, shape, split, -0.22, 0.18) * entries
    return jnp.clip(entries, min=-bound, max=bound).astype(kind)


def setup_inputs(seed: int = 0) -> dict:
    arg_keys = jax.random.split(jax.random.key(seed), 9)
    u_pre = scatter_about(arg_keys[0], (SEQS, SEQLEN, SGU_W), 1.0, 6.0, ((0, 4), (1, 8)))
    v_pre = scatter_about(arg_keys[1], (SEQS, SEQLEN, SGU_W), 1.0, 6.0, ((0, 4), (1, 8)))
    d_out = scatter_about(arg_keys[2], (SEQS, SEQLEN, D), 1.0, 6.0, ((0, 4), (1, 8)))
    w_mix = scatter_about(arg_keys[3], (GROUPS, BLOCK, BLOCK), BLOCK ** -0.5, 0.5)
    mix_bias = jnp.clip(1.0 + 0.18 * jax.random.normal(arg_keys[4], (GROUPS, BLOCK), jnp.float32), 0.1, 1.9)
    norm_gain = jnp.clip(1.0 + 0.18 * jax.random.normal(arg_keys[5], (GROUPS, CHANS), jnp.float32), 0.1, 1.9)
    norm_shift = scatter_about(arg_keys[6], (GROUPS, CHANS), 0.5, 3.0, (), jnp.float32)
    w_out = scatter_about(arg_keys[7], (SGU_W, D), SGU_W ** -0.5, 0.125, ((0, 4),))
    return {"u_pre": u_pre, "v_pre": v_pre, "d_out": d_out, "w_mix": w_mix, "mix_bias": mix_bias, "norm_gain": norm_gain, "norm_shift": norm_shift, "w_out": w_out}


EPS = 1e-05

def mechanism(grad_s, u_pre, v_pre, w_mix, mix_bias, gain, shift):
    items, length, width = grad_s.shape
    groups, span = (w_mix.shape[0], w_mix.shape[1])
    chans = width // groups
    shape = (items, length // span, span, groups, chans)
    u_val = u_pre.astype(jnp.float32).reshape(shape)
    v_val = v_pre.astype(jnp.float32).reshape(shape)
    cotan = grad_s.astype(jnp.float32).reshape(shape)
    upper, u_back = jax.vjp(jax.nn.gelu, u_val)
    gated, v_back = jax.vjp(jax.nn.gelu, v_val)
    centre = gated - lax.optimization_barrier(jnp.mean(gated, axis=-1, keepdims=True))
    inverse = lax.rsqrt(lax.optimization_barrier(jnp.mean(centre * centre, axis=-1, keepdims=True)) + EPS)
    scaled = centre * inverse
    normed = (scaled * gain + shift).astype(jnp.bfloat16)
    lower = jnp.tril(jnp.ones((span, span), dtype=bool))
    w_low = jnp.where(lower[None], w_mix, jnp.zeros_like(w_mix))
    mixed = jnp.einsum('gts,insgc->intgc', w_low.astype(jnp.float32), normed.astype(jnp.float32))
    mixed = mixed + jnp.transpose(mix_bias)[:, :, None]
    gated_out = (upper * mixed).astype(jnp.bfloat16)
    d_mixed = cotan * upper
    d_mixed_b = d_mixed.astype(jnp.bfloat16)
    grad_u = u_back(cotan * mixed)[0].astype(jnp.bfloat16).reshape(items, length, width)
    grad_bias = jnp.transpose(lax.optimization_barrier(jnp.sum(d_mixed, axis=(0, 1, 4))))
    grad_w = jnp.einsum('intgc,insgc->gts', d_mixed_b.astype(jnp.float32), normed.astype(jnp.float32))
    grad_w = jnp.where(lower[None], grad_w, jnp.zeros_like(grad_w))
    d_normed = jnp.einsum('gts,intgc->insgc', w_low.astype(jnp.float32), d_mixed_b.astype(jnp.float32))
    grad_gain = lax.optimization_barrier(jnp.sum(d_normed * scaled, axis=(0, 1, 2)))
    grad_shift = lax.optimization_barrier(jnp.sum(d_normed, axis=(0, 1, 2)))
    d_scaled = d_normed * gain
    d_gated = inverse * (d_scaled - lax.optimization_barrier(jnp.mean(d_scaled, axis=-1, keepdims=True)) - scaled * lax.optimization_barrier(jnp.mean(d_scaled * scaled, axis=-1, keepdims=True)))
    grad_v = v_back(d_gated)[0].astype(jnp.bfloat16).reshape(items, length, width)
    return (grad_u, grad_v, gated_out.reshape(items, length, width), grad_w, grad_bias, grad_gain, grad_shift)

def reference(u_pre, v_pre, d_out, w_mix, mix_bias, norm_gain, norm_shift, w_out):
    flat_d = d_out.reshape(-1, D)
    grad_s = jnp.dot(flat_d, jnp.transpose(w_out), preferred_element_type=jnp.float32)
    grad_s = grad_s.astype(jnp.bfloat16).reshape(SEQS, SEQLEN, SGU_W)

    def one_sequence(packed):
        cot, upre, vpre = packed
        return mechanism(cot[None], upre[None], vpre[None], w_mix, mix_bias, norm_gain, norm_shift)
    grad_u, grad_v, gated_out, grad_w, grad_bias, grad_gain, grad_shift = lax.map(one_sequence, (grad_s, u_pre, v_pre))
    grad_u = grad_u.reshape(SEQS, SEQLEN, SGU_W)
    grad_v = grad_v.reshape(SEQS, SEQLEN, SGU_W)
    flat_s = gated_out.reshape(-1, SGU_W)
    grad_w_out = jnp.dot(jnp.transpose(flat_s), flat_d, preferred_element_type=jnp.float32)
    return (grad_u, grad_v, grad_w_out, lax.optimization_barrier(jnp.sum(grad_w, axis=0)), lax.optimization_barrier(jnp.sum(grad_bias, axis=0)), lax.optimization_barrier(jnp.sum(grad_gain, axis=0)), lax.optimization_barrier(jnp.sum(grad_shift, axis=0)))
```

```python
import functools

import jax
import jax.numpy as jnp
from jax import lax
from jax.experimental import pallas as pl
from jax.experimental.pallas import tpu as pltpu
from jax.sharding import PartitionSpec as P

EPS = 1e-05
K0 = 0.7978845608028654
K1 = 0.044715
AXES = ("sp", "dp")
bf16 = jnp.bfloat16
f32 = jnp.float32


def swap(value, bit_sp, bit_dp):
    num_sp, num_dp = lax.axis_size("sp"), lax.axis_size("dp")
    pairs = [
        (s * num_dp + d, (s ^ bit_sp) * num_dp + (d ^ bit_dp))
        for s in range(num_sp)
        for d in range(num_dp)
    ]
    return lax.ppermute(value, AXES, pairs)


def dot(a, b, dims):
    return lax.dot_general(a, b, (dims, ((), ())), preferred_element_type=f32)


def forward_kernel(cfg, sc, u, v, d_out, w_low, bias, gain, shift, *rest):
    span, chans, per, piece, inner, fused = cfg
    if fused:
        recv, s1, k1, s2, k2, upper_o, m1_o, scaled_o, w1_o, gated = rest
    else:
        part, upper_o, m1_o, scaled_o, w1_o, gated = rest
    blocks = u.shape[0] // span
    cols = []
    for g in range(per):
        row = jnp.broadcast_to(bias[g], (chans, span))
        cols.append(jnp.transpose(row))

    def step(b, carry):
        rows = pl.ds(pl.multiple_of(b * span, span), span)
        for g in range(per):
            lanes = slice(g * chans, (g + 1) * chans)
            a = u[rows, lanes].astype(f32)
            c = v[rows, lanes].astype(f32)
            c2 = c * c
            tv = jnp.tanh(c * (K0 + (K0 * K1) * c2))
            hv = 0.5 + 0.5 * tv
            gate = c * hv
            dv = hv + (c * (0.5 - 0.5 * tv * tv)) * (K0 + (3.0 * K0 * K1) * c2)
            centre = gate - jnp.mean(gate, axis=1, keepdims=True)
            inv = lax.rsqrt(jnp.mean(centre * centre, axis=1, keepdims=True) + EPS)
            scaled = centre * inv
            normed = (scaled * gain[g] + shift[g]).astype(bf16)
            mixed = dot(w_low[g], normed, ((1,), (0,))) + cols[g]
            a2 = a * a
            tu = jnp.tanh(a * (K0 + (K0 * K1) * a2))
            hu = 0.5 + 0.5 * tu
            up = a * hu
            du = hu + (a * (0.5 - 0.5 * tu * tu)) * (K0 + (3.0 * K0 * K1) * a2)
            gated[rows, lanes] = (up * mixed).astype(bf16)
            upper_o[rows, lanes] = up.astype(bf16)
            m1_o[rows, lanes] = (mixed * du).astype(bf16)
            scaled_o[rows, lanes] = scaled.astype(bf16)
            w1_o[rows, lanes] = (dv * inv).astype(bf16)
        return carry

    lax.fori_loop(0, blocks, step, 0)
    if not fused:
        part[0] = dot(gated[...], d_out[...], ((0,), (0,))).astype(bf16)
        return
    half = d_out.shape[1] // 2
    count = per * chans // piece
    for side, (send, keep) in enumerate(((s1, k1), (s2, k2))):
        lanes = slice(side * half, (side + 1) * half)
        total = dot(gated[...], d_out[:, lanes], ((0,), (0,)))
        for p in range(count):
            rows = slice(p * piece, (p + 1) * piece)
            value = (total[rows] + recv[0, rows, lanes].astype(f32)).astype(bf16)
            rel = jnp.bitwise_xor(p, sc[1] % inner)
            low, high = rel % 2, rel // 2
            if side == 0:
                flag, at = low, high
            else:
                flag, at = high % 2, (high // 2) * 2 + low
            where = pl.ds(pl.multiple_of(at * piece, piece), piece)

            @pl.when(flag == 1)
            def _():
                send[0, where, :] = value

            @pl.when(flag == 0)
            def _():
                keep[0, where, :] = value


def forward(sc, u, v, d_out, w_low, bias, gain, shift, recv):
    num_sp, num_dp = lax.axis_size("sp"), lax.axis_size("dp")
    length, width = u.shape
    groups, span, _ = w_low.shape
    chans = width // groups
    rows = width // num_dp
    per = 2
    chunk = per * chans
    steps = rows // chunk
    count = num_dp // 2
    piece = rows // num_sp
    inner = chunk // piece
    fused = recv is not None
    first = num_dp - (2 if fused else 1)

    def at(i, j, sc):
        return jnp.bitwise_xor(first - 2 * i, sc[0]) * steps + j

    wide = pl.BlockSpec((length, chunk), lambda i, j, sc: (0, at(i, j, sc)))
    vec = pl.BlockSpec((per, 1, span), lambda i, j, sc: (at(i, j, sc), 0, 0))
    in_specs = [
        wide,
        wide,
        pl.BlockSpec(d_out.shape, lambda i, j, sc: (0, 0), pipeline_mode=pl.Buffered(1)),
        pl.BlockSpec((per, span, span), lambda i, j, sc: (at(i, j, sc), 0, 0)),
        vec,
        vec,
        vec,
    ]
    args = [u, v, d_out, w_low, bias, gain, shift]
    save = pl.BlockSpec((length, chunk), lambda i, j, sc: (0, i * steps + j))
    save_shape = jax.ShapeDtypeStruct((length, count * rows), bf16)
    depth = d_out.shape[1]
    if fused:
        in_specs.append(pl.BlockSpec((1, chunk, depth), lambda i, j, sc: (i, j, 0)))
        args.append(recv)
        spec = pl.BlockSpec(
            (1, chunk // 2, depth // 2),
            lambda i, j, sc: (i, jnp.bitwise_xor(j, sc[1] // inner), 0),
        )
        heads = [spec] * 4
        shapes = [jax.ShapeDtypeStruct((count, rows // 2, depth // 2), bf16)] * 4
    else:
        heads = [pl.BlockSpec((1, chunk, depth), lambda i, j, sc: (i, j, 0))]
        shapes = [jax.ShapeDtypeStruct((count, rows, depth), bf16)]
    return pl.pallas_call(
        functools.partial(forward_kernel, (span, chans, per, piece, inner, fused)),
        grid_spec=pltpu.PrefetchScalarGridSpec(
            num_scalar_prefetch=1,
            grid=(count, steps),
            in_specs=in_specs,
            out_specs=heads + [save] * 4,
            scratch_shapes=[pltpu.VMEM((length, chunk), bf16)],
        ),
        out_shape=shapes + [save_shape] * 4,
        name="forward_own" if fused else "forward_other",
    )(sc, *args)


def backward_kernel(cfg, sc, d_out, w, upper, m1, scaled_i, w1, w_up, gain, shift, *rest):
    span, chans, per = cfg
    gu, gv, small, grad = rest[-4:]
    blocks = upper.shape[0] // span
    grad[...] = dot(d_out[...], w[...], ((1,), (1,))).astype(bf16)

    def step(b, carry):
        rows = pl.ds(pl.multiple_of(b * span, span), span)
        out = []
        for g in range(per):
            acc_w, acc_b, acc_g, acc_s = carry[4 * g : 4 * g + 4]
            lanes = slice(g * chans, (g + 1) * chans)
            cot = grad[rows, lanes].astype(f32)
            gu[rows, lanes] = (cot * m1[rows, lanes].astype(f32)).astype(bf16)
            dm = cot * upper[rows, lanes].astype(f32)
            dmb = dm.astype(bf16)
            scaled = scaled_i[rows, lanes].astype(f32)
            normed = (scaled * gain[g] + shift[g]).astype(bf16)
            acc_w = acc_w + dot(dmb, normed, ((1,), (1,)))
            dn = dot(w_up[g], dmb, ((1,), (0,)))
            e = dn * gain[g]
            mean_e = jnp.mean(e, axis=1, keepdims=True)
            mean_s = jnp.mean(e * scaled, axis=1, keepdims=True)
            gv[rows, lanes] = (
                w1[rows, lanes].astype(f32) * (e - mean_e - scaled * mean_s)
            ).astype(bf16)
            out += [acc_w, acc_b + dm, acc_g + dn * scaled, acc_s + dn]
        return tuple(out)

    zero = jnp.zeros((span, chans), f32)
    done = lax.fori_loop(0, blocks, step, (zero,) * (4 * per))
    row = lax.broadcasted_iota(jnp.int32, (span, span), 0)
    col = lax.broadcasted_iota(jnp.int32, (span, span), 1)
    lines = []
    for g in range(per):
        lines.append(jnp.sum(jnp.transpose(done[4 * g + 1]), axis=0, keepdims=True))
        lines.append(jnp.sum(done[4 * g + 2], axis=0, keepdims=True))
        lines.append(jnp.sum(done[4 * g + 3], axis=0, keepdims=True))
    even, odd = done[0], done[4]
    diag = jnp.sum(jnp.where(row == col, odd, 0.0), axis=0, keepdims=True)
    small[0, :span] = jnp.where(row >= col, even, jnp.transpose(odd))
    pad = jnp.zeros((small.shape[1] - span - 7, span), f32)
    small[0, span:] = jnp.concatenate(lines + [diag, pad], axis=0)


SMALL_ROWS = 144


def backward(sc, rel, index, d_out, w, saves, w_up, gain, shift, carried):
    num_dp = lax.axis_size("dp")
    length, depth = d_out.shape
    groups, span, _ = w_up.shape
    rows = w.shape[0]
    width = rows * num_dp
    chans = width // groups
    per = 2
    chunk = per * chans
    steps = rows // chunk

    def at(j, sc):
        return jnp.bitwise_xor(rel, sc[0]) * steps + j

    save = pl.BlockSpec((length, chunk), lambda j, sc: (0, index * steps + j))
    vec = pl.BlockSpec((per, 1, span), lambda j, sc: (at(j, sc), 0, 0))
    in_specs = [
        pl.BlockSpec(d_out.shape, lambda j, sc: (0, 0), pipeline_mode=pl.Buffered(1)),
        pl.BlockSpec((chunk, depth), lambda j, sc: (j, 0)),
        save,
        save,
        save,
        save,
        pl.BlockSpec((per, span, span), lambda j, sc: (at(j, sc), 0, 0)),
        vec,
        vec,
    ]
    args = [d_out, w, *saves, w_up, gain, shift]
    aliases = {}
    if carried is not None:
        for k, value in enumerate(carried):
            aliases[1 + len(args)] = k
            in_specs.append(pl.BlockSpec(memory_space=pl.ANY))
            args.append(value)
    out = pl.BlockSpec((length, chunk), lambda j, sc: (0, at(j, sc)))
    shape = jax.ShapeDtypeStruct((length, width), bf16)
    return pl.pallas_call(
        functools.partial(backward_kernel, (span, chans, per)),
        grid_spec=pltpu.PrefetchScalarGridSpec(
            num_scalar_prefetch=1,
            grid=(steps,),
            in_specs=in_specs,
            out_specs=[
                out,
                out,
                pl.BlockSpec((1, SMALL_ROWS, span), lambda j, sc: (at(j, sc), 0, 0)),
            ],
            scratch_shapes=[pltpu.VMEM((length, chunk), bf16)],
        ),
        out_shape=[
            shape,
            shape,
            jax.ShapeDtypeStruct((groups // per, SMALL_ROWS, span), f32),
        ],
        input_output_aliases=aliases,
        name=f"backward_{rel}",
    )(sc, *args)


def assemble_kernel(sc, a, b, out):
    half = a.shape[-1]
    out[:, :half] = a[0].astype(f32)
    out[:, half:] = b[0].astype(f32)


def assemble(sc, first, second, order_a, order_b, rows):
    pieces, piece, half = first.shape

    def place(order):
        def index(p, sc):
            rel = jnp.bitwise_xor(p, sc[1])
            at = 0
            for bit in order:
                at = at * 2 + jnp.bitwise_and(rel // bit, 1)
            return (at, 0, 0)

        return index

    return pl.pallas_call(
        assemble_kernel,
        grid_spec=pltpu.PrefetchScalarGridSpec(
            num_scalar_prefetch=1,
            grid=(pieces,),
            in_specs=[
                pl.BlockSpec((1, piece, half), place(order_a)),
                pl.BlockSpec((1, piece, half), place(order_b)),
            ],
            out_specs=pl.BlockSpec((piece, 2 * half), lambda p, sc: (p, 0)),
        ),
        out_shape=jax.ShapeDtypeStruct((rows, 2 * half), f32),
        name="assemble",
    )(sc, first, second)


def bits_of(count):
    return [1 << k for k in range(count.bit_length() - 1)]


def add(a, b):
    return (a.astype(f32) + b.astype(f32)).astype(a.dtype)


def reduce_projection(sc, s1, k1, s2, k2, piece):
    num_sp, num_dp = lax.axis_size("sp"), lax.axis_size("dp")
    sp_bits = bits_of(num_sp)
    bit_a, bit_b, others = sp_bits[0], sp_bits[1], sp_bits[2:]
    count, _, half = k1.shape
    rest = num_sp // 4
    k1 = add(k1, swap(s1, bit_a, 0)).reshape(count, rest, 2, piece, half)
    k2 = add(k2, swap(s2, bit_b, 0)).reshape(count, rest, 2, piece, half)
    r1 = swap(k1[:, :, 1], bit_b, 0)
    r2 = swap(k2[:, :, 1], bit_a, 0)
    both = jnp.stack([add(k1[:, :, 0], r1), add(k2[:, :, 0], r2)], axis=1)
    for bit in reversed(bits_of(num_dp)[1:]):
        middle = both.shape[0] // 2
        both = add(both[middle:], swap(both[:middle], 0, bit))
    both = both[0]
    for k, bit in enumerate(others):
        shape = both.shape
        split = (2, rest >> (k + 1), 2, 1 << k, piece, half)
        got = jnp.flip(swap(both, bit, 0).reshape(split), axis=2).reshape(shape)
        both = add(both, got)
    a, b = both[0], both[1]
    a = jnp.concatenate([a, swap(a, bit_a, 0)], axis=0)
    b = jnp.concatenate([b, swap(b, bit_b, 0)], axis=0)
    a = jnp.concatenate([a, swap(a, bit_b, 0)], axis=0)
    b = jnp.concatenate([b, swap(b, bit_a, 0)], axis=0)
    high = list(reversed(others))
    return assemble(sc, a, b, [bit_b, bit_a] + high, [bit_a, bit_b] + high, num_sp * piece)


def reduce_small(value):
    steps = [(0, bit) for bit in bits_of(lax.axis_size("dp"))]
    steps += [(bit, 0) for bit in bits_of(lax.axis_size("sp"))]
    shape = value.shape
    value = value.reshape(-1, shape[-1])
    done = []
    for bit_sp, bit_dp in steps[:4]:
        if bit_dp:
            mine = jnp.bitwise_and(lax.axis_index("dp") // bit_dp, 1)
        else:
            mine = jnp.bitwise_and(lax.axis_index("sp") // bit_sp, 1)
        half = value.shape[0] // 2
        keep = lax.dynamic_slice_in_dim(value, mine * half, half)
        send = lax.dynamic_slice_in_dim(value, (1 - mine) * half, half)
        value = keep + swap(send, bit_sp, bit_dp)
        done.append((bit_sp, bit_dp, mine))
    for bit_sp, bit_dp in steps[4:]:
        value = value + swap(value, bit_sp, bit_dp)
    for bit_sp, bit_dp, mine in reversed(done):
        other = swap(value, bit_sp, bit_dp)
        first = jnp.where(mine == 0, value, other)
        second = jnp.where(mine == 0, other, value)
        value = jnp.concatenate([first, second], axis=0)
    return value.reshape(shape)


def on_device(u_pre, v_pre, d_out, w_mix, mix_bias, norm_gain, norm_shift, w_out):
    num_sp, num_dp = lax.axis_size("sp"), lax.axis_size("dp")
    shape = u_pre.shape
    width = shape[2]
    groups, span, _ = w_mix.shape
    u, v = u_pre.reshape(-1, width), v_pre.reshape(-1, width)
    d = d_out.reshape(-1, d_out.shape[2])
    sc = jnp.stack([lax.axis_index("dp"), lax.axis_index("sp")]).astype(jnp.int32)
    lower = jnp.tril(jnp.ones((span, span), dtype=bool))
    w_low = jnp.where(lower[None], w_mix, jnp.zeros_like(w_mix))
    w_up = jnp.swapaxes(w_low, 1, 2)
    bias, gain, shift = (a[:, None, :] for a in (mix_bias, norm_gain, norm_shift))

    weights = {0: w_out}
    for rel in range(2, num_dp, 2):
        top = 1 << (rel.bit_length() - 1)
        weights[rel] = swap(weights[rel - top], 0, top)
    for rel in range(0, num_dp, 2):
        weights[rel + 1] = swap(weights[rel], 0, 1)

    part, *saves_other = forward(sc, u, v, d, w_low, bias, gain, shift, None)
    recv = swap(part, 0, 1)
    s1, k1, s2, k2, *saves_own = forward(sc, u, v, d, w_low, bias, gain, shift, recv)
    carried = None
    order = [1, 0] + list(range(2, num_dp))
    for rel in order:
        saves = saves_own if rel % 2 == 0 else saves_other
        index = num_dp // 2 - 1 - rel // 2
        carried = backward(
            sc, rel, index, d, weights[rel], saves, w_up, gain, shift, carried
        )
    grad_u, grad_v, small = carried
    grad_w_out = reduce_projection(sc, s1, k1, s2, k2, width // num_dp // num_sp)
    small = reduce_small(small)
    body, lines = small[:, :span], small[:, span:]
    diag = jnp.where(jnp.eye(span, dtype=bool)[None], lines[:, 6][:, None, :], 0.0)
    strict = jnp.tril(jnp.ones((span, span), dtype=bool), -1)[None]
    even = jnp.where(lower[None], body, 0.0)
    odd = jnp.where(strict, jnp.swapaxes(body, 1, 2), diag)
    grad_w = jnp.stack([even, odd], axis=1).reshape(groups, span, span)
    lines = lines[:, :6].reshape(groups, 3, span)
    return (
        grad_u.reshape(shape),
        grad_v.reshape(shape),
        grad_w_out,
        grad_w,
        lines[:, 0],
        lines[:, 1],
        lines[:, 2],
    )


def solution(mesh):
    return jax.shard_map(
        on_device,
        mesh=mesh,
        in_specs=(
            P("dp", "sp", None),
            P("dp", "sp", None),
            P("dp", "sp", None),
            P(),
            P(),
            P(),
            P(),
            P("dp", None),
        ),
        out_specs=(P("dp", "sp", None), P("dp", "sp", None), P("dp", None), P(), P(), P(), P()),
        check_vma=False,
    )
```

```python
import functools

import jax
import jax.numpy as jnp
from jax import lax
from jax.experimental import pallas as pl
from jax.experimental.pallas import tpu as pltpu
from jax.sharding import PartitionSpec as P


EPS = 1e-05
K0 = 0.7978845608028654
K1 = 0.044715
VMEM = 18 << 20
AXES = ("sp", "dp")
bf16 = jnp.bfloat16
f32 = jnp.float32


def swap(value, bit_sp, bit_dp):
    num_sp, num_dp = lax.axis_size("sp"), lax.axis_size("dp")
    pairs = [
        (s * num_dp + d, (s ^ bit_sp) * num_dp + (d ^ bit_dp))
        for s in range(num_sp)
        for d in range(num_dp)
    ]
    return lax.ppermute(value, AXES, pairs)


def dot(a, b, dims):
    return lax.dot_general(a, b, (dims, ((), ())), preferred_element_type=f32)


def forward_kernel(cfg, sc, u, v, d_out, w_mix, bias, gain, shift, *rest):
    span, chans, per, piece, inner, fused = cfg
    if fused:
        recv, s1, k1, s2, k2, upper_o, m1_o, scaled_o, w1_o, gated, wide = rest
    else:
        part, upper_o, m1_o, scaled_o, w1_o, gated, wide = rest
    blocks = u.shape[0] // span

    row = lax.broadcasted_iota(jnp.int32, (span, span), 0)
    col = lax.broadcasted_iota(jnp.int32, (span, span), 1)
    for g in range(per):
        lanes = slice(g * chans, (g + 1) * chans)
        for b in range(blocks):
            rows = slice(b * span, (b + 1) * span)
            c = v[rows, lanes].astype(f32)
            c2 = c * c
            tv = jnp.tanh(c * (K0 + (K0 * K1) * c2))
            hv = 0.5 + 0.5 * tv
            gate = c * hv
            dv = hv + (c * (0.5 - 0.5 * tv * tv)) * (K0 + (3.0 * K0 * K1) * c2)
            centre = gate - jnp.mean(gate, axis=1, keepdims=True)
            var = jnp.mean(centre * centre, axis=1, keepdims=True)
            inv = lax.rsqrt(var + EPS)
            scaled = centre * inv
            wide[:, b * chans : (b + 1) * chans] = (scaled * gain[g] + shift[g]).astype(bf16)
            scaled_o[rows, lanes] = scaled.astype(bf16)
            w1_o[rows, lanes] = (dv * inv).astype(bf16)
        w_low = jnp.where(row >= col, w_mix[g], jnp.zeros_like(w_mix[g]))
        mixed_all = dot(w_low, wide[...], ((1,), (0,)))
        offset = jnp.transpose(jnp.broadcast_to(bias[g], (chans, span)))
        for b in range(blocks):
            rows = slice(b * span, (b + 1) * span)
            a = u[rows, lanes].astype(f32)
            mixed = mixed_all[:, b * chans : (b + 1) * chans] + offset
            a2 = a * a
            tu = jnp.tanh(a * (K0 + (K0 * K1) * a2))
            hu = 0.5 + 0.5 * tu
            up = a * hu
            du = hu + (a * (0.5 - 0.5 * tu * tu)) * (K0 + (3.0 * K0 * K1) * a2)
            gated[rows, lanes] = (up * mixed).astype(bf16)
            upper_o[rows, lanes] = up.astype(bf16)
            m1_o[rows, lanes] = (mixed * du).astype(bf16)
    if not fused:
        part[0] = dot(gated[...], d_out[...], ((0,), (0,))).astype(bf16)
        return
    half = d_out.shape[1] // 2
    count = per * chans // piece
    for side, (send, keep) in enumerate(((s1, k1), (s2, k2))):
        lanes = slice(side * half, (side + 1) * half)
        total = dot(gated[...], d_out[:, lanes], ((0,), (0,)))
        for p in range(count):
            rows = slice(p * piece, (p + 1) * piece)
            value = (total[rows] + recv[0, rows, lanes].astype(f32)).astype(bf16)
            rel = jnp.bitwise_xor(p, sc[1] % inner)
            low, high = rel % 2, rel // 2
            if side == 0:
                flag, at = low, high
            else:
                flag, at = high % 2, (high // 2) * 2 + low
            where = pl.ds(pl.multiple_of(at * piece, piece), piece)

            @pl.when(flag == 1)
            def _():
                send[0, where, :] = value

            @pl.when(flag == 0)
            def _():
                keep[0, where, :] = value


def forward(sc, first, count, u, v, d_out, w_mix, bias, gain, shift, recv):
    num_sp, num_dp = lax.axis_size("sp"), lax.axis_size("dp")
    length, width = u.shape
    groups, span, _ = w_mix.shape
    chans = width // groups
    rows = width // num_dp
    per = 2
    chunk = per * chans
    steps = rows // chunk
    piece = rows // num_sp
    inner = chunk // piece
    fused = recv is not None

    def at(i, j, sc):
        return jnp.bitwise_xor(first - 2 * i, sc[0]) * steps + j

    wide = pl.BlockSpec((length, chunk), lambda i, j, sc: (0, at(i, j, sc)))
    vec = pl.BlockSpec((per, 1, span), lambda i, j, sc: (at(i, j, sc), 0, 0))
    in_specs = [
        wide,
        wide,
        pl.BlockSpec(memory_space=pltpu.VMEM),
        pl.BlockSpec((per, span, span), lambda i, j, sc: (at(i, j, sc), 0, 0)),
        vec,
        vec,
        vec,
    ]
    args = [u, v, d_out, w_mix, bias, gain, shift]
    save = pl.BlockSpec((length, chunk), lambda i, j, sc: (0, i * steps + j))
    save_shape = jax.ShapeDtypeStruct((length, count * rows), bf16)
    depth = d_out.shape[1]
    if fused:
        in_specs.append(pl.BlockSpec((1, chunk, depth), lambda i, j, sc: (i, j, 0)))
        args.append(recv)
        spec = pl.BlockSpec(
            (1, chunk // 2, depth // 2),
            lambda i, j, sc: (i, jnp.bitwise_xor(j, sc[1] // inner), 0),
        )
        heads = [spec] * 4
        shapes = [jax.ShapeDtypeStruct((count, rows // 2, depth // 2), bf16)] * 4
    else:
        heads = [pl.BlockSpec((1, chunk, depth), lambda i, j, sc: (i, j, 0))]
        shapes = [jax.ShapeDtypeStruct((count, rows, depth), bf16)]
    return pl.pallas_call(
        functools.partial(forward_kernel, (span, chans, per, piece, inner, fused)),
        grid_spec=pltpu.PrefetchScalarGridSpec(
            num_scalar_prefetch=1,
            grid=(count, steps),
            in_specs=in_specs,
            out_specs=heads + [save] * 4,
            scratch_shapes=[
                pltpu.VMEM((length, chunk), bf16),
                pltpu.VMEM((span, length // span * chans), bf16),
            ],
        ),
        out_shape=shapes + [save_shape] * 4,
        cost_estimate=pl.CostEstimate(
            flops=2 * length * rows * count * depth, transcendentals=0, bytes_accessed=0
        ),
        compiler_params=pltpu.CompilerParams(vmem_limit_bytes=VMEM),
    )(sc, *args)


LINES = 16


def encode(ref, at, square, lines):
    span = square.shape[0]
    high = lines.astype(bf16)
    ref[at, :span] = square.astype(bf16)
    ref[at, span : span + LINES] = high
    ref[at, span + LINES :] = (lines - high.astype(f32)).astype(bf16)


def decode(ref, at):
    span = ref.shape[1] - 2 * LINES
    high = ref[at, span : span + LINES].astype(f32)
    return ref[at, :span].astype(f32), high + ref[at, span + LINES :].astype(f32)


def backward_kernel(cfg, sc, d_out, w, upper, m1, scaled_i, w1, w_mix, gain, shift, *rest):
    span, chans, per = cfg
    gu, gv, small, grad, dm_all, nm_all = rest[-6:]
    blocks = upper.shape[0] // span
    row = lax.broadcasted_iota(jnp.int32, (span, span), 0)
    col = lax.broadcasted_iota(jnp.int32, (span, span), 1)
    w_low = [jnp.where(row >= col, w_mix[g], jnp.zeros_like(w_mix[g])) for g in range(per)]
    nm_all[:, span:, :] = jnp.ones((per, span, nm_all.shape[2]), bf16)
    parts = 2
    acc = [None] * per
    acc_g = [jnp.zeros((8, chans), f32)] * per
    acc_s = [jnp.zeros((8, chans), f32)] * per
    size = blocks // parts
    for h in range(parts):
        grad[h * size * span : (h + 1) * size * span] = dot(d_out[h * size * span : (h + 1) * size * span], w[...], ((1,), (1,))).astype(bf16)
    for h in range(parts):
        wide = slice(h * size * chans, (h + 1) * size * chans)
        for g in range(per):
            lanes = slice(g * chans, (g + 1) * chans)
            for b in range(h * size, (h + 1) * size):
                rows = slice(b * span, (b + 1) * span)
                at = slice(b * chans, (b + 1) * chans)
                cot = grad[rows, lanes].astype(f32)
                gu[rows, lanes] = (cot * m1[rows, lanes].astype(f32)).astype(bf16)
                dm_all[g, :, at] = (cot * upper[rows, lanes].astype(f32)).astype(bf16)
                scaled = scaled_i[rows, lanes].astype(f32)
                nm_all[g, :span, at] = (scaled * gain[g] + shift[g]).astype(bf16)
            both = dot(dm_all[g, :, wide], nm_all[g, :, wide], ((1,), (1,)))
            acc[g] = both if h == 0 else acc[g] + both
            dn_all = dot(w_low[g], dm_all[g, :, wide], ((0,), (0,)))
            for b in range(h * size, (h + 1) * size):
                rows = slice(b * span, (b + 1) * span)
                k = b - h * size
                dn = dn_all[:, k * chans : (k + 1) * chans]
                scaled = scaled_i[rows, lanes].astype(f32)
                prod = dn * scaled
                acc_g[g] = acc_g[g] + jnp.sum(prod.reshape(-1, 8, chans), axis=0)
                acc_s[g] = acc_s[g] + jnp.sum(dn.reshape(-1, 8, chans), axis=0)
                e = dn * gain[g]
                mean_e = jnp.mean(e, axis=1, keepdims=True)
                mean_s = jnp.mean(prod * gain[g], axis=1, keepdims=True)
                gv[rows, lanes] = (
                    w1[rows, lanes].astype(f32) * (e - mean_e - scaled * mean_s)
                ).astype(bf16)
    lines, mats = [], []
    for g in range(per):
        mats.append(acc[g][:, :span])
        lines.append(jnp.transpose(acc[g][:, span:])[:1])
        lines.append(jnp.sum(acc_g[g], axis=0, keepdims=True))
        lines.append(jnp.sum(acc_s[g], axis=0, keepdims=True))
    even, odd = mats
    diag = jnp.sum(jnp.where(row == col, odd, 0.0), axis=0, keepdims=True)
    square = jnp.where(row >= col, even, jnp.transpose(odd))
    pad = jnp.zeros((LINES - 7, span), f32)
    lines = jnp.concatenate(lines + [diag, pad], axis=0)
    encode(small, 0, square, lines)


def backward(sc, rel, index, d_out, w, saves, w_mix, gain, shift, carried):
    num_dp = lax.axis_size("dp")
    length, depth = d_out.shape
    groups, span, _ = w_mix.shape
    rows = w.shape[0]
    width = rows * num_dp
    chans = width // groups
    per = 2
    chunk = per * chans
    steps = rows // chunk

    def at(j, sc):
        return jnp.bitwise_xor(rel, sc[0]) * steps + j

    save = pl.BlockSpec((length, chunk), lambda j, sc: (0, index * steps + j))
    vec = pl.BlockSpec((per, 1, span), lambda j, sc: (at(j, sc), 0, 0))
    in_specs = [
        pl.BlockSpec(memory_space=pltpu.VMEM),
        pl.BlockSpec((chunk, depth), lambda j, sc: (j, 0)),
        save,
        save,
        save,
        save,
        pl.BlockSpec((per, span, span), lambda j, sc: (at(j, sc), 0, 0)),
        vec,
        vec,
    ]
    args = [d_out, w, *saves, w_mix, gain, shift]
    aliases = {}
    if carried is not None:
        for k, value in enumerate(carried):
            aliases[1 + len(args)] = k
            in_specs.append(pl.BlockSpec(memory_space=pl.ANY))
            args.append(value)
    out = pl.BlockSpec((length, chunk), lambda j, sc: (0, at(j, sc)))
    shape = jax.ShapeDtypeStruct((length, width), bf16)
    return pl.pallas_call(
        functools.partial(backward_kernel, (span, chans, per)),
        grid_spec=pltpu.PrefetchScalarGridSpec(
            num_scalar_prefetch=1,
            grid=(steps,),
            in_specs=in_specs,
            out_specs=[
                out,
                out,
                pl.BlockSpec((1, span + 2 * LINES, span), lambda j, sc: (j, 0, 0)),
            ],
            scratch_shapes=[
                pltpu.VMEM((length, chunk), bf16),
                pltpu.VMEM((per, span, length // span * chans), bf16),
                pltpu.VMEM((per, 2 * span, length // span * chans), bf16),
            ],
        ),
        out_shape=[
            shape,
            shape,
            jax.ShapeDtypeStruct((steps, span + 2 * LINES, span), bf16),
        ],
        input_output_aliases=aliases,
        cost_estimate=pl.CostEstimate(
            flops=2 * length * rows * depth, transcendentals=0, bytes_accessed=0
        ),
        compiler_params=pltpu.CompilerParams(vmem_limit_bytes=VMEM),
    )(sc, *args)


def add(a, b):
    return (a.astype(f32) + b.astype(f32)).astype(bf16)


def split_kernel(k1, r1, k2, r2, send1, keep1, send2, keep2):
    for k, r, send, keep in ((k1, r1, send1, keep1), (k2, r2, send2, keep2)):
        for i in range(k.shape[0]):
            for j in range(k.shape[1]):
                send[i, j] = add(k[i, j, 1], r[i, j, 1])
                keep[i, j] = add(k[i, j, 0], r[i, j, 0])


def join_kernel(k1, r1, k2, r2, out):
    out[:, 0] = add(k1[...], r1[...])
    out[:, 1] = add(k2[...], r2[...])


def join_more_kernel(k1, r1, k2, r2, more, out):
    for side, (k, r) in enumerate(((k1, r1), (k2, r2))):
        total = k[...].astype(f32) + r[...].astype(f32)
        out[:, side] = (total + more[:, side].astype(f32)).astype(bf16)


def merge_kernel(mine, got, out):
    for i in range(mine.shape[0]):
        square, lines = decode(mine, i)
        more, extra = decode(got, i)
        encode(out, i, square + more, lines + extra)


def unpack_kernel(sc, *refs):
    *blocks, grad_w, bias, gain, shift = refs
    steps = blocks[0].shape[0]
    span = blocks[0].shape[2]
    row = lax.broadcasted_iota(jnp.int32, (span, span), 0)
    col = lax.broadcasted_iota(jnp.int32, (span, span), 1)
    for rel, block in enumerate(blocks):
        base = jnp.bitwise_xor(rel, sc[0]) * (2 * steps)
        for j in range(steps):
            square, lines = decode(block, j)
            even = jnp.where(row >= col, square, 0.0)
            odd = jnp.where(row > col, jnp.transpose(square), 0.0)
            odd = jnp.where(row == col, jnp.broadcast_to(lines[6:7], (span, span)), odd)
            for g, value in enumerate((even, odd)):
                at = base + 2 * j + g
                grad_w[at] = value
                for k, ref in enumerate((bias, gain, shift)):
                    ref[pl.ds(at, 1), :] = lines[3 * g + k : 3 * g + k + 1]


def unpack(sc, blocks, groups):
    span = blocks[0].shape[2]
    whole = pl.BlockSpec(memory_space=pltpu.VMEM)
    line = jax.ShapeDtypeStruct((groups, span), f32)
    return pl.pallas_call(
        unpack_kernel,
        in_specs=[pl.BlockSpec(memory_space=pltpu.SMEM)] + [whole] * len(blocks),
        out_specs=[whole] * 4,
        out_shape=[jax.ShapeDtypeStruct((groups, span, span), f32), line, line, line],
        compiler_params=pltpu.CompilerParams(vmem_limit_bytes=VMEM),
        name="unpack",
    )(sc, *blocks)


def flip_kernel(step, value, got, *outs):
    for side in range(value.shape[0]):
        for j in range(value.shape[1]):
            sums = add(value[side, j], got[side, j ^ step])
            if len(outs) == 1:
                outs[0][side, j] = sums
            else:
                outs[side][j] = sums


def local(body, shapes, *args):
    return pl.pallas_call(
        body,
        out_shape=[jax.ShapeDtypeStruct(shape, bf16) for shape in shapes],
        in_specs=[pl.BlockSpec(memory_space=pltpu.VMEM)] * len(args),
        out_specs=[pl.BlockSpec(memory_space=pltpu.VMEM)] * len(shapes),
        compiler_params=pltpu.CompilerParams(vmem_limit_bytes=VMEM),
    )(*args)


def assemble_kernel(sc, *refs):
    *parts, out = refs
    half = parts[0].shape[-1]
    piece = parts[0].shape[1]
    for side in range(2):
        for low in range(4):
            at = jnp.bitwise_xor(low, jnp.bitwise_and(sc[1], 3)) * piece
            rows = pl.ds(pl.multiple_of(at, piece), piece)
            lanes = slice(side * half, (side + 1) * half)
            out[rows, lanes] = parts[4 * side + low][0].astype(f32)


def assemble(sc, parts):
    rest, piece, half = parts[0].shape
    spec = pl.BlockSpec((1, piece, half), lambda h, sc: (jnp.bitwise_xor(h, sc[1] // 4), 0, 0))
    return pl.pallas_call(
        assemble_kernel,
        grid_spec=pltpu.PrefetchScalarGridSpec(
            num_scalar_prefetch=1,
            grid=(rest,),
            in_specs=[spec] * 8,
            out_specs=pl.BlockSpec((4 * piece, 2 * half), lambda h, sc: (h, 0)),
        ),
        out_shape=jax.ShapeDtypeStruct((rest * 4 * piece, 2 * half), f32),
        name="assemble",
    )(sc, *parts)


def bits_of(count):
    return [1 << k for k in range(count.bit_length() - 1)]


def reduce_small(packed):
    sp_bits, dp_bits = bits_of(lax.axis_size("sp")), bits_of(lax.axis_size("dp"))
    for bit in [dp_bits[0]] + list(reversed(dp_bits[1:])):
        for rel in [r for r in packed if r & bit]:
            got = swap(packed.pop(rel), 0, bit)
            mine = packed[rel ^ bit]
            packed[rel ^ bit] = local(merge_kernel, [mine.shape], mine, got)[0]
    value = packed[0]
    for bit in sp_bits:
        value = local(merge_kernel, [value.shape], value, swap(value, bit, 0))[0]
    blocks = {0: value}
    for bit in dp_bits[1:] + [dp_bits[0]]:
        for rel in list(blocks):
            blocks[rel | bit] = swap(blocks[rel], 0, bit)
    return [blocks[rel] for rel in range(len(blocks))]


def program(u_pre, v_pre, d_out, w_mix, mix_bias, norm_gain, norm_shift, w_out):
    num_sp, num_dp = lax.axis_size("sp"), lax.axis_size("dp")
    shape = u_pre.shape
    width = shape[2]
    groups, _, _ = w_mix.shape
    u, v = u_pre.reshape(-1, width), v_pre.reshape(-1, width)
    d = d_out.reshape(-1, d_out.shape[2])
    sc = jnp.stack([lax.axis_index("dp"), lax.axis_index("sp")]).astype(jnp.int32)
    bias, gain, shift = (a[:, None, :] for a in (mix_bias, norm_gain, norm_shift))
    u, v, w_mix, bias, gain, shift = (
        pltpu.with_memory_space_constraint(a, pltpu.HBM) for a in (u, v, w_mix, bias, gain, shift)
    )

    sp_bits, dp_bits = bits_of(num_sp), bits_of(num_dp)
    bit_a, bit_b, others = sp_bits[0], sp_bits[1], sp_bits[2:]
    piece = width // num_dp // num_sp
    depth = d.shape[1]
    half = depth // 2
    rest = num_sp // 4
    count = num_dp // 4
    weights = {0: w_out, 1: swap(w_out, 0, 1)}
    for rel in range(2, num_dp, 2):
        top = 1 << (rel.bit_length() - 1)
        weights[rel] = swap(weights[rel - top], 0, top)
    for rel in range(2, num_dp, 2):
        weights[rel + 1] = swap(weights[rel], 0, 1)

    saves, heads = {}, {}

    def front(rel, recv):
        out = forward(sc, rel, count, u, v, d, w_mix, bias, gain, shift, recv)
        kept = out[-4:]
        for i in range(count):
            saves[rel - 2 * i] = (kept, i)
        heads[rel] = out[:-4]

    packed = {}

    def back(rel, carried):
        kept, i = saves[rel]
        *carried, packed[rel] = backward(
            sc, rel, i, d, weights[rel], kept, w_mix, gain, shift, carried
        )
        return carried

    top, low = num_dp - 1, num_dp // 2 - 1
    front(top, None)
    recv_a = swap(heads[top][0], 0, 1)
    front(low, None)
    recv_b = swap(heads[low][0], 0, 1)
    front(top - 1, recv_a)
    s1a, k1a, s2a, k2a = heads[top - 1]
    r1a, r2a = swap(s1a, bit_a, 0), swap(s2a, bit_b, 0)
    front(low - 1, recv_b)
    s1b, k1b, s2b, k2b = heads[low - 1]
    r1b, r2b = swap(s1b, bit_a, 0), swap(s2b, bit_b, 0)
    shaped = (count, rest, 2, piece, half)
    done = (count, rest, piece, half)

    def split(*arrays):
        return local(split_kernel, [done] * 4, *(x.reshape(shaped) for x in arrays))

    carried = back(1, None)
    t1a, k1a, t2a, k2a = split(k1a, r1a, k2a, r2a)
    r1a, r2a = swap(t1a, bit_b, 0), swap(t2a, bit_a, 0)
    carried = back(2, carried)
    t1b, k1b, t2b, k2b = split(k1b, r1b, k2b, r2b)
    r1b, r2b = swap(t1b, bit_b, 0), swap(t2b, bit_a, 0)
    stacked = (count, 2, rest, piece, half)
    send = local(join_kernel, [stacked], k1a, r1a, k2a, r2a)[0]
    both_r = swap(send, 0, dp_bits[-1])
    carried = back(3, carried)
    both = local(join_more_kernel, [stacked], k1b, r1b, k2b, r2b, both_r)[0]
    for bit in reversed(dp_bits[1:-1]):
        middle = both.shape[0] // 2
        both = add(both[middle:], swap(both[:middle], 0, bit))
    both = both[0]
    for k, bit in enumerate(others):
        got = swap(both, bit, 0)
        if k == len(others) - 1:
            shapes = [(rest, piece, half)] * 2
            for rel in list(range(4, num_dp)) + [0]:
                carried = back(rel, carried)
        else:
            shapes = [both.shape]
        out = local(functools.partial(flip_kernel, 1 << k), shapes, both, got)
        both = out[0]
    a, b = out
    grad_u, grad_v = carried
    a1, b2 = swap(a, bit_a, 0), swap(b, bit_b, 0)
    a2, b1 = swap(a, bit_b, 0), swap(b, bit_a, 0)
    a3, b3 = swap(a1, bit_b, 0), swap(b2, bit_a, 0)
    grad_w_out = assemble(sc, [a, a1, a2, a3, b, b1, b2, b3])
    grads = unpack(sc, reduce_small(packed), groups)
    return (grad_u.reshape(shape), grad_v.reshape(shape), grad_w_out, *grads)


def solution(mesh):
    return jax.shard_map(
        program,
        mesh=mesh,
        in_specs=(
            P("dp", "sp", None),
            P("dp", "sp", None),
            P("dp", "sp", None),
            P(),
            P(),
            P(),
            P(),
            P("dp", None),
        ),
        out_specs=(P("dp", "sp", None), P("dp", "sp", None), P("dp", None), P(), P(), P(), P()),
        check_vma=False,
    )
```

```python
import functools

import jax
import jax.numpy as jnp
from jax import lax
from jax.experimental import pallas as pl
from jax.experimental.pallas import tpu as pltpu
from jax.sharding import PartitionSpec as P


EPS = 1e-05
K0 = 0.7978845608028654
K1 = 0.044715
VMEM = 18 << 20
AXES = ("sp", "dp")
bf16 = jnp.bfloat16
f32 = jnp.float32


def swap(value, bit_sp, bit_dp):
    num_sp, num_dp = lax.axis_size("sp"), lax.axis_size("dp")
    pairs = [
        (s * num_dp + d, (s ^ bit_sp) * num_dp + (d ^ bit_dp))
        for s in range(num_sp)
        for d in range(num_dp)
    ]
    return lax.ppermute(value, AXES, pairs)


def dot(a, b, dims):
    return lax.dot_general(a, b, (dims, ((), ())), preferred_element_type=f32)


def forward_kernel(cfg, sc, u, v, d_out, w_mix, bias, gain, shift, *rest):
    span, chans, per, piece, inner, fused, resident, place = cfg
    here = pl.program_id(0) * pl.num_programs(1) + pl.program_id(1)
    if fused:
        recv, s1, k1, s2, k2, upper_o, m1_o, scaled_o, w1_o, gated, wide = rest
    else:
        part, upper_o, m1_o, scaled_o, w1_o, gated, wide = rest
    blocks = u.shape[0] // span

    row = lax.broadcasted_iota(jnp.int32, (span, span), 0)
    col = lax.broadcasted_iota(jnp.int32, (span, span), 1)
    for g in range(per):
        lanes = slice(g * chans, (g + 1) * chans)
        source = lanes
        if resident:
            start = (place(pl.program_id(0), pl.program_id(1), sc) * per + g) * chans
            source = pl.ds(pl.multiple_of(start, chans), chans)
        for b in range(blocks):
            rows = slice(b * span, (b + 1) * span)
            c = v[rows, source].astype(f32)
            c2 = c * c
            tv = jnp.tanh(c * (K0 + (K0 * K1) * c2))
            hv = 0.5 + 0.5 * tv
            gate = c * hv
            dv = hv + (gate * (1.0 - hv)) * (2.0 * K0 + (6.0 * K0 * K1) * c2)
            centre = gate - jnp.mean(gate, axis=1, keepdims=True)
            var = jnp.mean(centre * centre, axis=1, keepdims=True)
            inv = lax.rsqrt(var + EPS)
            scaled = centre * inv
            wide[:, b * chans : (b + 1) * chans] = (scaled * gain[g] + shift[g]).astype(bf16)
            scaled_o[here, rows, lanes] = scaled.astype(bf16)
            w1_o[here, rows, lanes] = (dv * inv).astype(bf16)
        w_low = jnp.where(row >= col, w_mix[g], jnp.zeros_like(w_mix[g]))
        mixed_all = dot(w_low, wide[...], ((1,), (0,)))
        offset = jnp.transpose(jnp.broadcast_to(bias[g], (chans, span)))
        for b in range(blocks):
            rows = slice(b * span, (b + 1) * span)
            a = u[rows, source].astype(f32)
            mixed = mixed_all[:, b * chans : (b + 1) * chans] + offset
            a2 = a * a
            tu = jnp.tanh(a * (K0 + (K0 * K1) * a2))
            hu = 0.5 + 0.5 * tu
            up = a * hu
            du = hu + (up * (1.0 - hu)) * (2.0 * K0 + (6.0 * K0 * K1) * a2)
            gated[rows, lanes] = (up * mixed).astype(bf16)
            upper_o[here, rows, lanes] = up.astype(bf16)
            m1_o[here, rows, lanes] = (mixed * du).astype(bf16)
    if not fused:
        part[here] = dot(gated[...], d_out[...], ((0,), (0,))).astype(bf16)
        return
    half = d_out.shape[1] // 2
    count = per * chans // piece
    there = pl.program_id(0) * pl.num_programs(1) + jnp.bitwise_xor(pl.program_id(1), sc[1] // inner)
    for side, (send, keep) in enumerate(((s1, k1), (s2, k2))):
        lanes = slice(side * half, (side + 1) * half)
        total = dot(gated[...], d_out[:, lanes], ((0,), (0,)))
        for p in range(count):
            rows = slice(p * piece, (p + 1) * piece)
            value = (total[rows] + recv[here, rows, lanes].astype(f32)).astype(bf16)
            rel = jnp.bitwise_xor(p, sc[1] % inner)
            low, high = rel % 2, rel // 2
            if side == 0:
                flag, at = low, high
            else:
                flag, at = high % 2, (high // 2) * 2 + low
            where = pl.ds(pl.multiple_of(at * piece, piece), piece)

            @pl.when(flag == 1)
            def _():
                send[there, where, :] = value

            @pl.when(flag == 0)
            def _():
                keep[there, where, :] = value


def forward(sc, first, count, resident, u, v, d_out, w_mix, bias, gain, shift, recv):
    num_sp, num_dp = lax.axis_size("sp"), lax.axis_size("dp")
    length, width = u.shape
    groups, span, _ = w_mix.shape
    chans = width // groups
    rows = width // num_dp
    per = 2
    chunk = per * chans
    steps = rows // chunk
    piece = rows // num_sp
    inner = chunk // piece
    fused = recv is not None

    def at(i, j, sc):
        return jnp.bitwise_xor(first - 2 * i, sc[0]) * steps + j

    wide = pl.BlockSpec((length, chunk), lambda i, j, sc: (0, at(i, j, sc)))
    vec = pl.BlockSpec((per, 1, span), lambda i, j, sc: (at(i, j, sc), 0, 0))
    whole = pl.BlockSpec(memory_space=pltpu.VMEM)
    in_specs = [
        whole if resident else wide,
        whole if resident else wide,
        whole,
        pl.BlockSpec((per, span, span), lambda i, j, sc: (at(i, j, sc), 0, 0)),
        vec,
        vec,
        vec,
    ]
    args = [u, v, d_out, w_mix, bias, gain, shift]
    blocks = count * steps
    save_shape = jax.ShapeDtypeStruct((blocks, length, chunk), bf16)
    depth = d_out.shape[1]
    if fused:
        in_specs.append(whole)
        args.append(recv.reshape(blocks, chunk, depth))
        heads = [whole] * 4
        shapes = [jax.ShapeDtypeStruct((blocks, chunk // 2, depth // 2), bf16)] * 4
    else:
        heads = [whole]
        shapes = [jax.ShapeDtypeStruct((blocks, chunk, depth), bf16)]
    return pl.pallas_call(
        functools.partial(forward_kernel, (span, chans, per, piece, inner, fused, resident, at)),
        grid_spec=pltpu.PrefetchScalarGridSpec(
            num_scalar_prefetch=1,
            grid=(count, steps),
            in_specs=in_specs,
            out_specs=heads + [whole] * 4,
            scratch_shapes=[
                pltpu.VMEM((length, chunk), bf16),
                pltpu.VMEM((span, length // span * chans), bf16),
            ],
        ),
        out_shape=shapes + [save_shape] * 4,
        cost_estimate=pl.CostEstimate(
            flops=2 * length * rows * count * depth, transcendentals=0, bytes_accessed=0
        ),
        compiler_params=pltpu.CompilerParams(vmem_limit_bytes=VMEM),
    )(sc, *args)


LINES = 16


def encode(ref, at, square, lines):
    span = square.shape[0]
    high = lines.astype(bf16)
    ref[at, :span] = square.astype(bf16)
    ref[at, span : span + LINES] = high
    ref[at, span + LINES :] = (lines - high.astype(f32)).astype(bf16)


def decode(ref, at):
    span = ref.shape[1] - 2 * LINES
    high = ref[at, span : span + LINES].astype(f32)
    return ref[at, :span].astype(f32), high + ref[at, span + LINES :].astype(f32)


def backward_kernel(cfg, sc, d_out, w, upper, m1, scaled_i, w1, w_mix, gain, shift, *rest):
    span, chans, per, base = cfg
    here = pl.program_id(0)
    save = base + here
    gu, gv, small, grad, dm_all, nm_all = rest[-6:]
    blocks = upper.shape[1] // span
    row = lax.broadcasted_iota(jnp.int32, (span, span), 0)
    col = lax.broadcasted_iota(jnp.int32, (span, span), 1)
    w_low = [jnp.where(row >= col, w_mix[g], jnp.zeros_like(w_mix[g])) for g in range(per)]
    nm_all[:, span:, :] = jnp.ones((per, span, nm_all.shape[2]), bf16)
    parts = 2
    acc = [None] * per
    acc_g = [jnp.zeros((8, chans), f32)] * per
    acc_s = [jnp.zeros((8, chans), f32)] * per
    size = blocks // parts
    for h in range(parts):
        grad[h * size * span : (h + 1) * size * span] = dot(d_out[h * size * span : (h + 1) * size * span], w[here], ((1,), (1,))).astype(bf16)
    for h in range(parts):
        wide = slice(h * size * chans, (h + 1) * size * chans)
        for g in range(per):
            lanes = slice(g * chans, (g + 1) * chans)
            for b in range(h * size, (h + 1) * size):
                rows = slice(b * span, (b + 1) * span)
                at = slice(b * chans, (b + 1) * chans)
                cot = grad[rows, lanes].astype(f32)
                gu[rows, lanes] = (cot * m1[save, rows, lanes].astype(f32)).astype(bf16)
                dm_all[g, :, at] = (cot * upper[save, rows, lanes].astype(f32)).astype(bf16)
                scaled = scaled_i[save, rows, lanes].astype(f32)
                nm_all[g, :span, at] = (scaled * gain[g] + shift[g]).astype(bf16)
            both = dot(dm_all[g, :, wide], nm_all[g, :, wide], ((1,), (1,)))
            acc[g] = both if h == 0 else acc[g] + both
            dn_all = dot(w_low[g], dm_all[g, :, wide], ((0,), (0,)))
            for b in range(h * size, (h + 1) * size):
                rows = slice(b * span, (b + 1) * span)
                k = b - h * size
                dn = dn_all[:, k * chans : (k + 1) * chans]
                scaled = scaled_i[save, rows, lanes].astype(f32)
                prod = dn * scaled
                acc_g[g] = acc_g[g] + jnp.sum(prod.reshape(-1, 8, chans), axis=0)
                acc_s[g] = acc_s[g] + jnp.sum(dn.reshape(-1, 8, chans), axis=0)
                e = dn * gain[g]
                mean_e = jnp.mean(e, axis=1, keepdims=True)
                mean_s = jnp.mean(prod * gain[g], axis=1, keepdims=True)
                gv[rows, lanes] = (
                    w1[save, rows, lanes].astype(f32) * (e - mean_e - scaled * mean_s)
                ).astype(bf16)
    lines, mats = [], []
    for g in range(per):
        mats.append(acc[g][:, :span])
        lines.append(jnp.transpose(acc[g][:, span:])[:1])
        lines.append(jnp.sum(acc_g[g], axis=0, keepdims=True))
        lines.append(jnp.sum(acc_s[g], axis=0, keepdims=True))
    even, odd = mats
    diag = jnp.sum(jnp.where(row == col, odd, 0.0), axis=0, keepdims=True)
    square = jnp.where(row >= col, even, jnp.transpose(odd))
    pad = jnp.zeros((LINES - 7, span), f32)
    lines = jnp.concatenate(lines + [diag, pad], axis=0)
    encode(small, here, square, lines)


def backward(sc, rel, index, d_out, w, saves, w_mix, gain, shift, carried):
    num_dp = lax.axis_size("dp")
    length, depth = d_out.shape
    groups, span, _ = w_mix.shape
    rows = w.shape[0]
    width = rows * num_dp
    chans = width // groups
    per = 2
    chunk = per * chans
    steps = rows // chunk

    def at(j, sc):
        return jnp.bitwise_xor(rel, sc[0]) * steps + j

    whole = pl.BlockSpec(memory_space=pltpu.VMEM)
    vec = pl.BlockSpec((per, 1, span), lambda j, sc: (at(j, sc), 0, 0))
    in_specs = [whole] * 6 + [
        pl.BlockSpec((per, span, span), lambda j, sc: (at(j, sc), 0, 0)),
        vec,
        vec,
    ]
    args = [d_out, w.reshape(steps, chunk, depth), *saves, w_mix, gain, shift]
    aliases = {}
    if carried is not None:
        for k, value in enumerate(carried):
            aliases[1 + len(args)] = k
            in_specs.append(pl.BlockSpec(memory_space=pl.ANY))
            args.append(value)
    out = pl.BlockSpec((length, chunk), lambda j, sc: (0, at(j, sc)))
    shape = jax.ShapeDtypeStruct((length, width), bf16)
    return pl.pallas_call(
        functools.partial(backward_kernel, (span, chans, per, index * steps)),
        grid_spec=pltpu.PrefetchScalarGridSpec(
            num_scalar_prefetch=1,
            grid=(steps,),
            in_specs=in_specs,
            out_specs=[
                out,
                out,
                whole,
            ],
            scratch_shapes=[
                pltpu.VMEM((length, chunk), bf16),
                pltpu.VMEM((per, span, length // span * chans), bf16),
                pltpu.VMEM((per, 2 * span, length // span * chans), bf16),
            ],
        ),
        out_shape=[
            shape,
            shape,
            jax.ShapeDtypeStruct((steps, span + 2 * LINES, span), bf16),
        ],
        input_output_aliases=aliases,
        cost_estimate=pl.CostEstimate(
            flops=2 * length * rows * depth, transcendentals=0, bytes_accessed=0
        ),
        compiler_params=pltpu.CompilerParams(vmem_limit_bytes=VMEM),
    )(sc, *args)


def add(a, b):
    return (a.astype(f32) + b.astype(f32)).astype(bf16)


def split_kernel(k1, r1, k2, r2, send1, keep1, send2, keep2):
    for k, r, send, keep in ((k1, r1, send1, keep1), (k2, r2, send2, keep2)):
        for i in range(k.shape[0]):
            for j in range(k.shape[1]):
                send[i, j] = add(k[i, j, 1], r[i, j, 1])
                keep[i, j] = add(k[i, j, 0], r[i, j, 0])


def join_kernel(k, r, out):
    out[...] = add(k[...], r[...])


def join_more_kernel(k, r, more, out):
    total = k[...].astype(f32) + r[...].astype(f32)
    out[...] = (total + more[...].astype(f32)).astype(bf16)


def merge_kernel(mine, got, out):
    for i in range(mine.shape[0]):
        square, lines = decode(mine, i)
        more, extra = decode(got, i)
        encode(out, i, square + more, lines + extra)


def unpack_kernel(sc, *refs):
    *blocks, grad_w, bias, gain, shift = refs
    steps = blocks[0].shape[0]
    span = blocks[0].shape[2]
    row = lax.broadcasted_iota(jnp.int32, (span, span), 0)
    col = lax.broadcasted_iota(jnp.int32, (span, span), 1)
    for rel, block in enumerate(blocks):
        base = jnp.bitwise_xor(rel, sc[0]) * (2 * steps)
        for j in range(steps):
            square, lines = decode(block, j)
            even = jnp.where(row >= col, square, 0.0)
            odd = jnp.where(row > col, jnp.transpose(square), 0.0)
            odd = jnp.where(row == col, jnp.broadcast_to(lines[6:7], (span, span)), odd)
            for g, value in enumerate((even, odd)):
                at = base + 2 * j + g
                grad_w[at] = value
                for k, ref in enumerate((bias, gain, shift)):
                    ref[pl.ds(at, 1), :] = lines[3 * g + k : 3 * g + k + 1]


def unpack(sc, blocks, groups):
    span = blocks[0].shape[2]
    whole = pl.BlockSpec(memory_space=pltpu.VMEM)
    line = jax.ShapeDtypeStruct((groups, span), f32)
    return pl.pallas_call(
        unpack_kernel,
        in_specs=[pl.BlockSpec(memory_space=pltpu.SMEM)] + [whole] * len(blocks),
        out_specs=[whole] * 4,
        out_shape=[jax.ShapeDtypeStruct((groups, span, span), f32), line, line, line],
        compiler_params=pltpu.CompilerParams(vmem_limit_bytes=VMEM),
        name="unpack",
    )(sc, *blocks)


def flip_kernel(step, value, got, out):
    for j in range(value.shape[0]):
        out[j] = add(value[j], got[j ^ step])


def local(body, shapes, *args):
    return pl.pallas_call(
        body,
        out_shape=[jax.ShapeDtypeStruct(shape, bf16) for shape in shapes],
        in_specs=[pl.BlockSpec(memory_space=pltpu.VMEM)] * len(args),
        out_specs=[pl.BlockSpec(memory_space=pltpu.VMEM)] * len(shapes),
        compiler_params=pltpu.CompilerParams(vmem_limit_bytes=VMEM),
    )(*args)


def assemble_kernel(sc, *refs):
    parts, out = refs[:4], refs[-1]
    rest, piece, _ = parts[0].shape
    for low in range(4):
        for high in range(rest):
            at = jnp.bitwise_xor(4 * high + low, sc[1]) * piece
            out[pl.ds(pl.multiple_of(at, piece), piece), :] = parts[low][high].astype(f32)


def assemble(sc, side, parts, carried):
    rest, piece, half = parts[0].shape
    in_specs = [pl.BlockSpec(memory_space=pltpu.VMEM)] * 4
    args = list(parts)
    if carried is not None:
        in_specs.append(pl.BlockSpec(memory_space=pl.ANY))
        args.append(carried)
    return pl.pallas_call(
        assemble_kernel,
        grid_spec=pltpu.PrefetchScalarGridSpec(
            num_scalar_prefetch=1,
            grid=(1,),
            in_specs=in_specs,
            out_specs=pl.BlockSpec((rest * 4 * piece, half), lambda p, sc: (0, side)),
        ),
        out_shape=jax.ShapeDtypeStruct((rest * 4 * piece, 2 * half), f32),
        input_output_aliases={} if carried is None else {5: 0},
        compiler_params=pltpu.CompilerParams(vmem_limit_bytes=VMEM),
    )(sc, *args)


def bits_of(count):
    return [1 << k for k in range(count.bit_length() - 1)]


def reduce_small(packed):
    sp_bits, dp_bits = bits_of(lax.axis_size("sp")), bits_of(lax.axis_size("dp"))
    for bit in [dp_bits[0]] + list(reversed(dp_bits[1:])):
        for rel in [r for r in packed if r & bit]:
            got = swap(packed.pop(rel), 0, bit)
            mine = packed[rel ^ bit]
            packed[rel ^ bit] = local(merge_kernel, [mine.shape], mine, got)[0]
    value = packed[0]
    for bit in sp_bits:
        got = swap(value, bit, 0)
        value = local(merge_kernel, [value.shape], value, got)[0]
    blocks = {0: value}
    for bit in dp_bits[1:] + [dp_bits[0]]:
        for rel in list(blocks):
            blocks[rel | bit] = swap(blocks[rel], 0, bit)
    return [blocks[rel] for rel in range(len(blocks))]


def program(u_pre, v_pre, d_out, w_mix, mix_bias, norm_gain, norm_shift, w_out):
    num_sp, num_dp = lax.axis_size("sp"), lax.axis_size("dp")
    shape = u_pre.shape
    width = shape[2]
    groups, _, _ = w_mix.shape
    u, v = u_pre.reshape(-1, width), v_pre.reshape(-1, width)
    d = d_out.reshape(-1, d_out.shape[2])
    sc = jnp.stack([lax.axis_index("dp"), lax.axis_index("sp")]).astype(jnp.int32)
    bias, gain, shift = (a[:, None, :] for a in (mix_bias, norm_gain, norm_shift))
    u_far, v_far, w_mix, bias, gain, shift = (
        pltpu.with_memory_space_constraint(a, pltpu.HBM)
        for a in (u, v, w_mix, bias, gain, shift)
    )

    sp_bits, dp_bits = bits_of(num_sp), bits_of(num_dp)
    bit_a, bit_b, others = sp_bits[0], sp_bits[1], sp_bits[2:]
    piece = width // num_dp // num_sp
    depth = d.shape[1]
    half = depth // 2
    rest = num_sp // 4
    count = num_dp // 4
    weights = {0: w_out, 1: swap(w_out, 0, 1)}
    for rel in range(2, num_dp, 2):
        top = 1 << (rel.bit_length() - 1)
        weights[rel] = swap(weights[rel - top], 0, top)
    for rel in range(2, num_dp, 2):
        weights[rel + 1] = swap(weights[rel], 0, 1)

    saves, heads = {}, {}

    def front(rel, recv):
        if rel == num_dp - 1:
            big = (False, u_far, v_far, d)
        else:
            big = (True, u, v, d)
        out = forward(sc, rel, count, *big, w_mix, bias, gain, shift, recv)
        kept = out[-4:]
        for i in range(count):
            saves[rel - 2 * i] = (kept, i)
        heads[rel] = out[:-4]

    packed = {}

    def back(rel, carried):
        kept, i = saves[rel]
        *carried, packed[rel] = backward(
            sc, rel, i, d, weights[rel], kept, w_mix, gain, shift, carried
        )
        return carried

    top, low = num_dp - 1, num_dp // 2 - 1
    front(top, None)
    recv_a = swap(heads[top][0], 0, 1)
    front(low, None)
    recv_b = swap(heads[low][0], 0, 1)
    front(top - 1, recv_a)
    s1a, k1a, s2a, k2a = heads[top - 1]
    r1a, r2a = swap(s1a, bit_a, 0), swap(s2a, bit_b, 0)
    front(low - 1, recv_b)
    s1b, k1b, s2b, k2b = heads[low - 1]
    r1b, r2b = swap(s1b, bit_a, 0), swap(s2b, bit_b, 0)
    shaped = (count, rest, 2, piece, half)
    done = (count, rest, piece, half)

    def split(*arrays):
        return local(split_kernel, [done] * 4, *(x.reshape(shaped) for x in arrays))

    carried = back(1, None)
    t1a, k1a, t2a, k2a = split(k1a, r1a, k2a, r2a)
    r1a, r2a = swap(t1a, bit_b, 0), swap(t2a, bit_a, 0)
    carried = back(2, carried)
    t1b, k1b, t2b, k2b = split(k1b, r1b, k2b, r2b)
    r1b, r2b = swap(t1b, bit_b, 0), swap(t2b, bit_a, 0)
    ends_a, ends_b = ((k1a, r1a), (k2a, r2a)), ((k1b, r1b), (k2b, r2b))
    chip = []
    for pair in ends_a:
        send = local(join_kernel, [done], *pair)[0]
        chip.append(swap(send, 0, dp_bits[-1]))
    carried = back(3, carried)
    sides = [local(join_more_kernel, [done], *pair, x)[0] for pair, x in zip(ends_b, chip)]
    for bit in reversed(dp_bits[1:-1]):
        middle = sides[0].shape[0] // 2
        sides = [add(x[middle:], swap(x[:middle], 0, bit)) for x in sides]
    sides = [x[0] for x in sides]
    for k, bit in enumerate(others):
        got = [swap(x, bit, 0) for x in sides]
        if k == len(others) - 1:
            for rel in list(range(4, num_dp)) + [0]:
                carried = back(rel, carried)
        flip = functools.partial(flip_kernel, 1 << k)
        sides = [local(flip, [x.shape], x, y)[0] for x, y in zip(sides, got)]
    grad_u, grad_v = carried
    grad_w_out = None
    for side, (x, near, far) in enumerate(zip(sides, (bit_a, bit_b), (bit_b, bit_a))):
        one, two = swap(x, near, 0), swap(x, far, 0)
        three = swap(one, far, 0)
        middle = (one, two) if near == bit_a else (two, one)
        grad_w_out = assemble(sc, side, [x, *middle, three], grad_w_out)
    small = reduce_small(packed)
    grads = unpack(sc, small, groups)
    return (grad_u.reshape(shape), grad_v.reshape(shape), grad_w_out, *grads)


def solution(mesh):
    return jax.shard_map(
        program,
        mesh=mesh,
        in_specs=(
            P("dp", "sp", None),
            P("dp", "sp", None),
            P("dp", "sp", None),
            P(),
            P(),
            P(),
            P(),
            P("dp", None),
        ),
        out_specs=(P("dp", "sp", None), P("dp", "sp", None), P("dp", None), P(), P(), P(), P()),
        check_vma=False,
    )
```

```python
import functools

import jax
import jax.numpy as jnp
from jax import lax
from jax.experimental import pallas as pl
from jax.experimental.pallas import tpu as pltpu
from jax.sharding import PartitionSpec as P


EPS = 1e-05
K0 = 0.7978845608028654
K1 = 0.044715
VMEM = 18 << 20
AXES = ("sp", "dp")
bf16 = jnp.bfloat16
f32 = jnp.float32


def swap(value, bit_sp, bit_dp):
    num_sp, num_dp = lax.axis_size("sp"), lax.axis_size("dp")
    pairs = [
        (s * num_dp + d, (s ^ bit_sp) * num_dp + (d ^ bit_dp))
        for s in range(num_sp)
        for d in range(num_dp)
    ]
    return lax.ppermute(value, AXES, pairs)


def dot(a, b, dims):
    return lax.dot_general(a, b, (dims, ((), ())), preferred_element_type=f32)


def forward_kernel(cfg, sc, u, v, d_out, w_mix, bias, gain, shift, *rest):
    span, chans, per, piece, inner, fused, resident, place = cfg
    here = pl.program_id(0) * pl.num_programs(1) + pl.program_id(1)
    if fused:
        recv, s1, k1, s2, k2, upper_o, m1_o, scaled_o, w1_o, gated, wide = rest
    else:
        part, upper_o, m1_o, scaled_o, w1_o, gated, wide = rest
    blocks = u.shape[0] // span
    first = place(pl.program_id(0), pl.program_id(1), sc) * per
    base = first if resident else 0

    row = lax.broadcasted_iota(jnp.int32, (span, span), 0)
    col = lax.broadcasted_iota(jnp.int32, (span, span), 1)
    for g in range(per):
        lanes = slice(g * chans, (g + 1) * chans)
        source = lanes
        if resident:
            source = pl.ds(pl.multiple_of((first + g) * chans, chans), chans)
        for b in range(blocks):
            rows = slice(b * span, (b + 1) * span)
            c = v[rows, source].astype(f32)
            c2 = c * c
            tv = jnp.tanh(c * (K0 + (K0 * K1) * c2))
            hv = 0.5 + 0.5 * tv
            gate = c * hv
            dv = hv + (gate * (1.0 - hv)) * (2.0 * K0 + (6.0 * K0 * K1) * c2)
            centre = gate - jnp.mean(gate, axis=1, keepdims=True)
            var = jnp.mean(centre * centre, axis=1, keepdims=True)
            inv = lax.rsqrt(var + EPS)
            scaled = centre * inv
            wide[:, b * chans : (b + 1) * chans] = (scaled * gain[base + g] + shift[base + g]).astype(bf16)
            scaled_o[here, rows, lanes] = scaled.astype(bf16)
            w1_o[here, rows, lanes] = (dv * inv).astype(bf16)
        w_low = w_mix[base + g]
        w_low = jnp.where(row >= col, w_low, jnp.zeros_like(w_low))
        mixed_all = dot(w_low, wide[...], ((1,), (0,)))
        offset = jnp.transpose(jnp.broadcast_to(bias[base + g], (chans, span)))
        for b in range(blocks):
            rows = slice(b * span, (b + 1) * span)
            a = u[rows, source].astype(f32)
            mixed = mixed_all[:, b * chans : (b + 1) * chans] + offset
            a2 = a * a
            tu = jnp.tanh(a * (K0 + (K0 * K1) * a2))
            hu = 0.5 + 0.5 * tu
            up = a * hu
            du = hu + (up * (1.0 - hu)) * (2.0 * K0 + (6.0 * K0 * K1) * a2)
            gated[rows, lanes] = (up * mixed).astype(bf16)
            upper_o[here, rows, lanes] = up.astype(bf16)
            m1_o[here, rows, lanes] = (mixed * du).astype(bf16)
    if not fused:
        part[here] = dot(gated[...], d_out[...], ((0,), (0,))).astype(bf16)
        return
    half = d_out.shape[1] // 2
    own = sc[1] % inner
    there = pl.program_id(0) * pl.num_programs(1) + jnp.bitwise_xor(pl.program_id(1), sc[1] // inner)
    for side, (send, keep) in enumerate(((s1, k1), (s2, k2))):
        lanes = slice(side * half, (side + 1) * half)
        total = dot(gated[...], d_out[:, lanes], ((0,), (0,)))
        total = (total + recv[here, :, lanes].astype(f32)).astype(bf16)
        swapped = jnp.bitwise_and(own // (1 << side), 1) == 1
        for p in range(per * chans // piece):
            if p & (1 << side):
                continue
            q = p + (1 << side)
            low = total[p * piece : (p + 1) * piece]
            high = total[q * piece : (q + 1) * piece]
            rel = jnp.bitwise_xor(p, own)
            at = rel // 2 if side == 0 else rel // 4 * 2 + rel % 2
            where = pl.ds(pl.multiple_of(at * piece, piece), piece)
            send[there, where, :] = jnp.where(swapped, low, high)
            keep[there, where, :] = jnp.where(swapped, high, low)


def forward(sc, first, count, resident, u, v, d_out, w_mix, bias, gain, shift, recv):
    num_sp, num_dp = lax.axis_size("sp"), lax.axis_size("dp")
    length, width = u.shape
    groups, span, _ = w_mix.shape
    chans = width // groups
    rows = width // num_dp
    per = 2
    chunk = per * chans
    steps = rows // chunk
    piece = rows // num_sp
    inner = chunk // piece
    fused = recv is not None

    def at(i, j, sc):
        return jnp.bitwise_xor(first - 2 * i, sc[0]) * steps + j

    wide = pl.BlockSpec((length, chunk), lambda i, j, sc: (0, at(i, j, sc)))
    whole = pl.BlockSpec(memory_space=pltpu.VMEM)
    in_specs = [
        whole if resident else wide,
        whole if resident else wide,
        whole,
    ]
    if resident:
        in_specs += [whole] * 4
    else:
        in_specs.append(pl.BlockSpec((per, span, span), lambda i, j, sc: (at(i, j, sc), 0, 0)))
        in_specs += [pl.BlockSpec((per, 1, span), lambda i, j, sc: (at(i, j, sc), 0, 0))] * 3
    args = [u, v, d_out, w_mix, bias, gain, shift]
    blocks = count * steps
    save_shape = jax.ShapeDtypeStruct((blocks, length, chunk), bf16)
    depth = d_out.shape[1]
    if fused:
        in_specs.append(whole)
        args.append(recv.reshape(blocks, chunk, depth))
        heads = [whole] * 4
        shapes = [jax.ShapeDtypeStruct((blocks, chunk // 2, depth // 2), bf16)] * 4
    else:
        heads = [whole]
        shapes = [jax.ShapeDtypeStruct((blocks, chunk, depth), bf16)]
    return pl.pallas_call(
        functools.partial(forward_kernel, (span, chans, per, piece, inner, fused, resident, at)),
        grid_spec=pltpu.PrefetchScalarGridSpec(
            num_scalar_prefetch=1,
            grid=(count, steps),
            in_specs=in_specs,
            out_specs=heads + [whole] * 4,
            scratch_shapes=[
                pltpu.VMEM((length, chunk), bf16),
                pltpu.VMEM((span, length // span * chans), bf16),
            ],
        ),
        out_shape=shapes + [save_shape] * 4,
        cost_estimate=pl.CostEstimate(
            flops=2 * length * rows * count * depth, transcendentals=0, bytes_accessed=0
        ),
        compiler_params=pltpu.CompilerParams(vmem_limit_bytes=VMEM),
    )(sc, *args)


LINES = 16


def encode(ref, at, square, lines):
    span = square.shape[0]
    high = lines.astype(bf16)
    ref[at, :span] = square.astype(bf16)
    ref[at, span : span + LINES] = high
    ref[at, span + LINES :] = (lines - high.astype(f32)).astype(bf16)


def decode(ref, at):
    span = ref.shape[1] - 2 * LINES
    high = ref[at, span : span + LINES].astype(f32)
    return ref[at, :span].astype(f32), high + ref[at, span + LINES :].astype(f32)


def backward_kernel(cfg, sc, d_out, w, upper, m1, scaled_i, w1, w_mix, gain, shift, *rest):
    span, chans, per, base, place = cfg
    here = pl.program_id(0)
    first = place(here, sc) * per
    save = base + here
    gu, gv, small, grad, dm_all, nm_all = rest[-6:]
    blocks = upper.shape[1] // span
    row = lax.broadcasted_iota(jnp.int32, (span, span), 0)
    col = lax.broadcasted_iota(jnp.int32, (span, span), 1)
    w_low = [w_mix[first + g] for g in range(per)]
    w_low = [jnp.where(row >= col, m, jnp.zeros_like(m)) for m in w_low]
    nm_all[:, span:, :] = jnp.ones((per, span, nm_all.shape[2]), bf16)
    parts = 2
    acc = [None] * per
    acc_g = [jnp.zeros((8, chans), f32)] * per
    acc_s = [jnp.zeros((8, chans), f32)] * per
    size = blocks // parts
    for h in range(parts):
        grad[h * size * span : (h + 1) * size * span] = dot(d_out[h * size * span : (h + 1) * size * span], w[here], ((1,), (1,))).astype(bf16)
    for h in range(parts):
        wide = slice(h * size * chans, (h + 1) * size * chans)
        for g in range(per):
            lanes = slice(g * chans, (g + 1) * chans)
            for b in range(h * size, (h + 1) * size):
                rows = slice(b * span, (b + 1) * span)
                at = slice(b * chans, (b + 1) * chans)
                cot = grad[rows, lanes].astype(f32)
                gu[rows, lanes] = (cot * m1[save, rows, lanes].astype(f32)).astype(bf16)
                dm_all[g, :, at] = (cot * upper[save, rows, lanes].astype(f32)).astype(bf16)
                scaled = scaled_i[save, rows, lanes].astype(f32)
                nm_all[g, :span, at] = (scaled * gain[first + g] + shift[first + g]).astype(bf16)
            both = dot(dm_all[g, :, wide], nm_all[g, :, wide], ((1,), (1,)))
            acc[g] = both if h == 0 else acc[g] + both
            dn_all = dot(w_low[g], dm_all[g, :, wide], ((0,), (0,)))
            for b in range(h * size, (h + 1) * size):
                rows = slice(b * span, (b + 1) * span)
                k = b - h * size
                dn = dn_all[:, k * chans : (k + 1) * chans]
                scaled = scaled_i[save, rows, lanes].astype(f32)
                prod = dn * scaled
                acc_g[g] = acc_g[g] + jnp.sum(prod.reshape(-1, 8, chans), axis=0)
                acc_s[g] = acc_s[g] + jnp.sum(dn.reshape(-1, 8, chans), axis=0)
                e = dn * gain[first + g]
                mean_e = jnp.mean(e, axis=1, keepdims=True)
                mean_s = jnp.mean(prod * gain[first + g], axis=1, keepdims=True)
                gv[rows, lanes] = (
                    w1[save, rows, lanes].astype(f32) * (e - mean_e - scaled * mean_s)
                ).astype(bf16)
    lines, mats = [], []
    for g in range(per):
        mats.append(acc[g][:, :span])
        lines.append(jnp.transpose(acc[g][:, span:])[:1])
        lines.append(jnp.sum(acc_g[g], axis=0, keepdims=True))
        lines.append(jnp.sum(acc_s[g], axis=0, keepdims=True))
    even, odd = mats
    diag = jnp.sum(jnp.where(row == col, odd, 0.0), axis=0, keepdims=True)
    square = jnp.where(row >= col, even, jnp.transpose(odd))
    pad = jnp.zeros((LINES - 7, span), f32)
    lines = jnp.concatenate(lines + [diag, pad], axis=0)
    encode(small, here, square, lines)


def backward(sc, rel, index, d_out, w, saves, w_mix, gain, shift, carried):
    num_dp = lax.axis_size("dp")
    length, depth = d_out.shape
    groups, span, _ = w_mix.shape
    rows = w.shape[0]
    width = rows * num_dp
    chans = width // groups
    per = 2
    chunk = per * chans
    steps = rows // chunk

    def at(j, sc):
        return jnp.bitwise_xor(rel, sc[0]) * steps + j

    whole = pl.BlockSpec(memory_space=pltpu.VMEM)
    in_specs = [whole] * 9
    args = [d_out, w.reshape(steps, chunk, depth), *saves, w_mix, gain, shift]
    aliases = {}
    if carried is not None:
        for k, value in enumerate(carried):
            aliases[1 + len(args)] = k
            in_specs.append(pl.BlockSpec(memory_space=pl.ANY))
            args.append(value)
    out = pl.BlockSpec((length, chunk), lambda j, sc: (0, at(j, sc)))
    shape = jax.ShapeDtypeStruct((length, width), bf16)
    return pl.pallas_call(
        functools.partial(backward_kernel, (span, chans, per, index * steps, at)),
        grid_spec=pltpu.PrefetchScalarGridSpec(
            num_scalar_prefetch=1,
            grid=(steps,),
            in_specs=in_specs,
            out_specs=[
                out,
                out,
                whole,
            ],
            scratch_shapes=[
                pltpu.VMEM((length, chunk), bf16),
                pltpu.VMEM((per, span, length // span * chans), bf16),
                pltpu.VMEM((per, 2 * span, length // span * chans), bf16),
            ],
        ),
        out_shape=[
            shape,
            shape,
            jax.ShapeDtypeStruct((steps, span + 2 * LINES, span), bf16),
        ],
        input_output_aliases=aliases,
        cost_estimate=pl.CostEstimate(
            flops=2 * length * rows * depth, transcendentals=0, bytes_accessed=0
        ),
        compiler_params=pltpu.CompilerParams(vmem_limit_bytes=VMEM),
    )(sc, *args)


def add(a, b):
    return (a.astype(f32) + b.astype(f32)).astype(bf16)


def split_kernel(k1, r1, k2, r2, send1, keep1, send2, keep2):
    for k, r, send, keep in ((k1, r1, send1, keep1), (k2, r2, send2, keep2)):
        for i in range(k.shape[0]):
            for j in range(k.shape[1]):
                send[i, j] = add(k[i, j, 1], r[i, j, 1])
                keep[i, j] = add(k[i, j, 0], r[i, j, 0])


def join_kernel(k, r, out):
    out[...] = add(k[...], r[...])


def join_more_kernel(k, r, more, out):
    total = k[...].astype(f32) + r[...].astype(f32)
    out[...] = (total + more[...].astype(f32)).astype(bf16)


def merge_kernel(mine, got, out):
    for i in range(mine.shape[0]):
        square, lines = decode(mine, i)
        more, extra = decode(got, i)
        encode(out, i, square + more, lines + extra)


def unpack_kernel(sc, *refs):
    *blocks, grad_w, bias, gain, shift = refs
    steps = blocks[0].shape[0]
    span = blocks[0].shape[2]
    row = lax.broadcasted_iota(jnp.int32, (span, span), 0)
    col = lax.broadcasted_iota(jnp.int32, (span, span), 1)
    for rel, block in enumerate(blocks):
        base = jnp.bitwise_xor(rel, sc[0]) * (2 * steps)
        for j in range(steps):
            square, lines = decode(block, j)
            even = jnp.where(row >= col, square, 0.0)
            odd = jnp.where(row > col, jnp.transpose(square), 0.0)
            odd = jnp.where(row == col, jnp.broadcast_to(lines[6:7], (span, span)), odd)
            for g, value in enumerate((even, odd)):
                at = base + 2 * j + g
                grad_w[at] = value
                for k, ref in enumerate((bias, gain, shift)):
                    ref[pl.ds(at, 1), :] = lines[3 * g + k : 3 * g + k + 1]


def unpack(sc, blocks, groups):
    span = blocks[0].shape[2]
    whole = pl.BlockSpec(memory_space=pltpu.VMEM)
    line = jax.ShapeDtypeStruct((groups, span), f32)
    return pl.pallas_call(
        unpack_kernel,
        in_specs=[pl.BlockSpec(memory_space=pltpu.SMEM)] + [whole] * len(blocks),
        out_specs=[whole] * 4,
        out_shape=[jax.ShapeDtypeStruct((groups, span, span), f32), line, line, line],
        compiler_params=pltpu.CompilerParams(vmem_limit_bytes=VMEM),
        name="unpack",
    )(sc, *blocks)


def flip_kernel(step, value, got, out):
    for j in range(value.shape[0]):
        out[j] = add(value[j], got[j ^ step])


def local(body, shapes, *args):
    return pl.pallas_call(
        body,
        out_shape=[jax.ShapeDtypeStruct(shape, bf16) for shape in shapes],
        in_specs=[pl.BlockSpec(memory_space=pltpu.VMEM)] * len(args),
        out_specs=[pl.BlockSpec(memory_space=pltpu.VMEM)] * len(shapes),
        compiler_params=pltpu.CompilerParams(vmem_limit_bytes=VMEM),
    )(*args)


def assemble_kernel(sc, *refs):
    parts, out = refs[:4], refs[-1]
    rest, piece, _ = parts[0].shape
    for low in range(4):
        for high in range(rest):
            at = jnp.bitwise_xor(4 * high + low, sc[1]) * piece
            out[pl.ds(pl.multiple_of(at, piece), piece), :] = parts[low][high].astype(f32)


def assemble(sc, side, parts, carried):
    rest, piece, half = parts[0].shape
    in_specs = [pl.BlockSpec(memory_space=pltpu.VMEM)] * 4
    args = list(parts)
    if carried is not None:
        in_specs.append(pl.BlockSpec(memory_space=pl.ANY))
        args.append(carried)
    return pl.pallas_call(
        assemble_kernel,
        grid_spec=pltpu.PrefetchScalarGridSpec(
            num_scalar_prefetch=1,
            grid=(1,),
            in_specs=in_specs,
            out_specs=pl.BlockSpec((rest * 4 * piece, half), lambda p, sc: (0, side)),
        ),
        out_shape=jax.ShapeDtypeStruct((rest * 4 * piece, 2 * half), f32),
        input_output_aliases={} if carried is None else {5: 0},
        compiler_params=pltpu.CompilerParams(vmem_limit_bytes=VMEM),
    )(sc, *args)


def bits_of(count):
    return [1 << k for k in range(count.bit_length() - 1)]


def reduce_small(packed):
    sp_bits, dp_bits = bits_of(lax.axis_size("sp")), bits_of(lax.axis_size("dp"))
    for bit in [dp_bits[0]] + list(reversed(dp_bits[1:])):
        for rel in [r for r in packed if r & bit]:
            got = swap(packed.pop(rel), 0, bit)
            mine = packed[rel ^ bit]
            packed[rel ^ bit] = local(merge_kernel, [mine.shape], mine, got)[0]
    value = packed[0]
    for bit in sp_bits:
        got = swap(value, bit, 0)
        value = local(merge_kernel, [value.shape], value, got)[0]
    blocks = {0: value}
    for bit in dp_bits[1:] + [dp_bits[0]]:
        for rel in list(blocks):
            blocks[rel | bit] = swap(blocks[rel], 0, bit)
    return [blocks[rel] for rel in range(len(blocks))]


def program(u_pre, v_pre, d_out, w_mix, mix_bias, norm_gain, norm_shift, w_out):
    num_sp, num_dp = lax.axis_size("sp"), lax.axis_size("dp")
    shape = u_pre.shape
    width = shape[2]
    groups, _, _ = w_mix.shape
    u, v = u_pre.reshape(-1, width), v_pre.reshape(-1, width)
    d = d_out.reshape(-1, d_out.shape[2])
    sc = jnp.stack([lax.axis_index("dp"), lax.axis_index("sp")]).astype(jnp.int32)
    bias, gain, shift = (a[:, None, :] for a in (mix_bias, norm_gain, norm_shift))
    small = (w_mix, bias, gain, shift)
    u_far, v_far, *small_far = (
        pltpu.with_memory_space_constraint(a, pltpu.HBM) for a in (u, v, *small)
    )

    sp_bits, dp_bits = bits_of(num_sp), bits_of(num_dp)
    bit_a, bit_b, others = sp_bits[0], sp_bits[1], sp_bits[2:]
    piece = width // num_dp // num_sp
    depth = d.shape[1]
    half = depth // 2
    rest = num_sp // 4
    count = num_dp // 4
    weights = {0: w_out, 1: swap(w_out, 0, 1)}
    for rel in range(2, num_dp, 2):
        top = 1 << (rel.bit_length() - 1)
        weights[rel] = swap(weights[rel - top], 0, top)
    for rel in range(2, num_dp, 2):
        weights[rel + 1] = swap(weights[rel], 0, 1)

    saves, heads = {}, {}

    def front(rel, recv):
        if rel == num_dp - 1:
            out = forward(sc, rel, count, False, u_far, v_far, d, *small_far, recv)
        else:
            out = forward(sc, rel, count, True, u, v, d, *small, recv)
        kept = out[-4:]
        for i in range(count):
            saves[rel - 2 * i] = (kept, i)
        heads[rel] = out[:-4]

    packed = {}

    def back(rel, carried):
        kept, i = saves[rel]
        *carried, packed[rel] = backward(
            sc, rel, i, d, weights[rel], kept, w_mix, gain, shift, carried
        )
        return carried

    top, low = num_dp - 1, num_dp // 2 - 1
    front(top, None)
    recv_a = swap(heads[top][0], 0, 1)
    front(low, None)
    recv_b = swap(heads[low][0], 0, 1)
    front(top - 1, recv_a)
    s1a, k1a, s2a, k2a = heads[top - 1]
    r1a, r2a = swap(s1a, bit_a, 0), swap(s2a, bit_b, 0)
    front(low - 1, recv_b)
    s1b, k1b, s2b, k2b = heads[low - 1]
    r1b, r2b = swap(s1b, bit_a, 0), swap(s2b, bit_b, 0)
    shaped = (count, rest, 2, piece, half)
    done = (count, rest, piece, half)

    def split(*arrays):
        return local(split_kernel, [done] * 4, *(x.reshape(shaped) for x in arrays))

    carried = back(1, None)
    t1a, k1a, t2a, k2a = split(k1a, r1a, k2a, r2a)
    r1a, r2a = swap(t1a, bit_b, 0), swap(t2a, bit_a, 0)
    carried = back(0, carried)
    t1b, k1b, t2b, k2b = split(k1b, r1b, k2b, r2b)
    r1b, r2b = swap(t1b, bit_b, 0), swap(t2b, bit_a, 0)
    ends_a, ends_b = ((k1a, r1a), (k2a, r2a)), ((k1b, r1b), (k2b, r2b))
    chip = []
    for pair in ends_a:
        send = local(join_kernel, [done], *pair)[0]
        chip.append(swap(send, 0, dp_bits[-1]))
    carried = back(2, carried)
    sides = [local(join_more_kernel, [done], *pair, x)[0] for pair, x in zip(ends_b, chip)]
    for bit in reversed(dp_bits[1:-1]):
        middle = sides[0].shape[0] // 2
        sides = [add(x[middle:], swap(x[:middle], 0, bit)) for x in sides]
    sides = [x[0] for x in sides]
    for k, bit in enumerate(others):
        got = [swap(x, bit, 0) for x in sides]
        if k == len(others) - 1:
            for rel in range(3, num_dp):
                carried = back(rel, carried)
        flip = functools.partial(flip_kernel, 1 << k)
        sides = [local(flip, [x.shape], x, y)[0] for x, y in zip(sides, got)]
    grad_u, grad_v = carried
    pieces = []
    for x, near, far in zip(sides, (bit_a, bit_b), (bit_b, bit_a)):
        one, two = swap(x, near, 0), swap(x, far, 0)
        three = swap(one, far, 0)
        middle = (one, two) if near == bit_a else (two, one)
        pieces.append([x, *middle, three])
    grad_w_out = None
    for side in (1, 0):
        grad_w_out = assemble(sc, side, pieces[side], grad_w_out)
    sums = reduce_small(packed)
    grads = unpack(sc, sums, groups)
    return (grad_u.reshape(shape), grad_v.reshape(shape), grad_w_out, *grads)


def solution(mesh):
    return jax.shard_map(
        program,
        mesh=mesh,
        in_specs=(
            P("dp", "sp", None),
            P("dp", "sp", None),
            P("dp", "sp", None),
            P(),
            P(),
            P(),
            P(),
            P("dp", None),
        ),
        out_specs=(P("dp", "sp", None), P("dp", "sp", None), P("dp", None), P(), P(), P(), P()),
        check_vma=False,
    )
```

```python
import functools

import jax
import jax.numpy as jnp
from jax import lax
from jax.experimental import pallas as pl
from jax.experimental.pallas import tpu as pltpu
from jax.sharding import PartitionSpec as P


EPS = 1e-05
K0 = 0.7978845608028654
K1 = 0.044715
VMEM = 18 << 20
AXES = ("sp", "dp")
bf16 = jnp.bfloat16
f32 = jnp.float32


def swap(value, bit_sp, bit_dp):
    num_sp, num_dp = lax.axis_size("sp"), lax.axis_size("dp")
    pairs = [
        (s * num_dp + d, (s ^ bit_sp) * num_dp + (d ^ bit_dp))
        for s in range(num_sp)
        for d in range(num_dp)
    ]
    return lax.ppermute(value, AXES, pairs)


def dot(a, b, dims):
    return lax.dot_general(a, b, (dims, ((), ())), preferred_element_type=f32)


def forward_kernel(cfg, sc, u, v, d_out, w_mix, bias, gain, shift, *rest):
    span, chans, per, piece, inner, fused, resident, place = cfg
    here = pl.program_id(0) * pl.num_programs(1) + pl.program_id(1)
    if fused:
        recv, s1, k1, s2, k2, upper_o, m1_o, scaled_o, w1_o, gated, wide = rest
    else:
        part, upper_o, m1_o, scaled_o, w1_o, gated, wide = rest
    blocks = u.shape[0] // span
    first = place(pl.program_id(0), pl.program_id(1), sc) * per
    base = first if resident else 0

    row = lax.broadcasted_iota(jnp.int32, (span, span), 0)
    col = lax.broadcasted_iota(jnp.int32, (span, span), 1)
    for g in range(per):
        lanes = slice(g * chans, (g + 1) * chans)
        source = lanes
        if resident:
            source = pl.ds(pl.multiple_of((first + g) * chans, chans), chans)
        for b in range(blocks):
            rows = slice(b * span, (b + 1) * span)
            c = v[rows, source].astype(f32)
            c2 = c * c
            tv = jnp.tanh(c * (K0 + (K0 * K1) * c2))
            hv = 0.5 + 0.5 * tv
            gate = c * hv
            dv = hv + (gate * (1.0 - hv)) * (2.0 * K0 + (6.0 * K0 * K1) * c2)
            centre = gate - jnp.mean(gate, axis=1, keepdims=True)
            var = jnp.mean(centre * centre, axis=1, keepdims=True)
            inv = lax.rsqrt(var + EPS)
            scaled = centre * inv
            wide[:, b * chans : (b + 1) * chans] = (scaled * gain[base + g] + shift[base + g]).astype(bf16)
            scaled_o[here, rows, lanes] = scaled.astype(bf16)
            w1_o[here, rows, lanes] = (dv * inv).astype(bf16)
        w_low = w_mix[base + g]
        w_low = jnp.where(row >= col, w_low, jnp.zeros_like(w_low))
        mixed_all = dot(w_low, wide[...], ((1,), (0,)))
        offset = jnp.transpose(jnp.broadcast_to(bias[base + g], (chans, span)))
        for b in range(blocks):
            rows = slice(b * span, (b + 1) * span)
            a = u[rows, source].astype(f32)
            mixed = mixed_all[:, b * chans : (b + 1) * chans] + offset
            a2 = a * a
            tu = jnp.tanh(a * (K0 + (K0 * K1) * a2))
            hu = 0.5 + 0.5 * tu
            up = a * hu
            du = hu + (up * (1.0 - hu)) * (2.0 * K0 + (6.0 * K0 * K1) * a2)
            gated[rows, lanes] = (up * mixed).astype(bf16)
            upper_o[here, rows, lanes] = up.astype(bf16)
            m1_o[here, rows, lanes] = (mixed * du).astype(bf16)
    if not fused:
        part[here] = dot(gated[...], d_out[...], ((0,), (0,))).astype(bf16)
        return
    half = d_out.shape[1] // 2
    own = sc[1] % inner
    there = pl.program_id(0) * pl.num_programs(1) + jnp.bitwise_xor(pl.program_id(1), sc[1] // inner)
    for side, (send, keep) in enumerate(((s1, k1), (s2, k2))):
        lanes = slice(side * half, (side + 1) * half)
        total = dot(gated[...], d_out[:, lanes], ((0,), (0,)))
        total = (total + recv[here, :, lanes].astype(f32)).astype(bf16)
        swapped = jnp.bitwise_and(own // (1 << side), 1) == 1
        for p in range(per * chans // piece):
            if p & (1 << side):
                continue
            q = p + (1 << side)
            low = total[p * piece : (p + 1) * piece]
            high = total[q * piece : (q + 1) * piece]
            rel = jnp.bitwise_xor(p, own)
            at = rel // 2 if side == 0 else rel // 4 * 2 + rel % 2
            where = pl.ds(pl.multiple_of(at * piece, piece), piece)
            send[there, where, :] = jnp.where(swapped, low, high)
            keep[there, where, :] = jnp.where(swapped, high, low)


def forward(sc, first, count, resident, u, v, d_out, w_mix, bias, gain, shift, recv):
    num_sp, num_dp = lax.axis_size("sp"), lax.axis_size("dp")
    length, width = u.shape
    groups, span, _ = w_mix.shape
    chans = width // groups
    rows = width // num_dp
    per = 2
    chunk = per * chans
    steps = rows // chunk
    piece = rows // num_sp
    inner = chunk // piece
    fused = recv is not None

    def at(i, j, sc):
        return jnp.bitwise_xor(first - 2 * i, sc[0]) * steps + j

    wide = pl.BlockSpec((length, chunk), lambda i, j, sc: (0, at(i, j, sc)))
    whole = pl.BlockSpec(memory_space=pltpu.VMEM)
    in_specs = [
        whole if resident else wide,
        whole if resident else wide,
        whole,
    ]
    if resident:
        in_specs += [whole] * 4
    else:
        in_specs.append(pl.BlockSpec((per, span, span), lambda i, j, sc: (at(i, j, sc), 0, 0)))
        in_specs += [pl.BlockSpec((per, 1, span), lambda i, j, sc: (at(i, j, sc), 0, 0))] * 3
    args = [u, v, d_out, w_mix, bias, gain, shift]
    blocks = count * steps
    save_shape = jax.ShapeDtypeStruct((blocks, length, chunk), bf16)
    depth = d_out.shape[1]
    if fused:
        in_specs.append(whole)
        args.append(recv.reshape(blocks, chunk, depth))
        heads = [whole] * 4
        shapes = [jax.ShapeDtypeStruct((blocks, chunk // 2, depth // 2), bf16)] * 4
    else:
        heads = [whole]
        shapes = [jax.ShapeDtypeStruct((blocks, chunk, depth), bf16)]
    return pl.pallas_call(
        functools.partial(forward_kernel, (span, chans, per, piece, inner, fused, resident, at)),
        grid_spec=pltpu.PrefetchScalarGridSpec(
            num_scalar_prefetch=1,
            grid=(count, steps),
            in_specs=in_specs,
            out_specs=heads + [whole] * 4,
            scratch_shapes=[
                pltpu.VMEM((length, chunk), bf16),
                pltpu.VMEM((span, length // span * chans), bf16),
            ],
        ),
        out_shape=shapes + [save_shape] * 4,
        cost_estimate=pl.CostEstimate(
            flops=2 * length * rows * count * depth, transcendentals=0, bytes_accessed=0
        ),
        compiler_params=pltpu.CompilerParams(vmem_limit_bytes=VMEM),
    )(sc, *args)


LINES = 16


def encode(ref, at, square, lines):
    span = square.shape[0]
    high = lines.astype(bf16)
    ref[at, :span] = square.astype(bf16)
    ref[at, span : span + LINES] = high
    ref[at, span + LINES :] = (lines - high.astype(f32)).astype(bf16)


def decode(ref, at):
    span = ref.shape[1] - 2 * LINES
    high = ref[at, span : span + LINES].astype(f32)
    return ref[at, :span].astype(f32), high + ref[at, span + LINES :].astype(f32)


def backward_kernel(cfg, sc, d_out, w, upper, m1, scaled_i, w1, w_mix, gain, shift, *rest):
    span, chans, per, base, place = cfg
    here = pl.program_id(0)
    first = place(here, sc) * per
    save = base + here
    gu, gv, small, grad, dm_all, nm_all = rest[-6:]
    blocks = upper.shape[1] // span
    row = lax.broadcasted_iota(jnp.int32, (span, span), 0)
    col = lax.broadcasted_iota(jnp.int32, (span, span), 1)
    w_low = [w_mix[first + g] for g in range(per)]
    w_low = [jnp.where(row >= col, m, jnp.zeros_like(m)) for m in w_low]
    nm_all[:, span:, :] = jnp.ones((per, span, nm_all.shape[2]), bf16)
    parts = 2
    acc = [None] * per
    acc_g = [jnp.zeros((8, chans), f32)] * per
    acc_s = [jnp.zeros((8, chans), f32)] * per
    size = blocks // parts
    for h in range(parts):
        grad[h * size * span : (h + 1) * size * span] = dot(d_out[h * size * span : (h + 1) * size * span], w[here], ((1,), (1,))).astype(bf16)
    for h in range(parts):
        wide = slice(h * size * chans, (h + 1) * size * chans)
        for g in range(per):
            lanes = slice(g * chans, (g + 1) * chans)
            for b in range(h * size, (h + 1) * size):
                rows = slice(b * span, (b + 1) * span)
                at = slice(b * chans, (b + 1) * chans)
                cot = grad[rows, lanes].astype(f32)
                gu[rows, lanes] = (cot * m1[save, rows, lanes].astype(f32)).astype(bf16)
                dm_all[g, :, at] = (cot * upper[save, rows, lanes].astype(f32)).astype(bf16)
                scaled = scaled_i[save, rows, lanes].astype(f32)
                nm_all[g, :span, at] = (scaled * gain[first + g] + shift[first + g]).astype(bf16)
            both = dot(dm_all[g, :, wide], nm_all[g, :, wide], ((1,), (1,)))
            acc[g] = both if h == 0 else acc[g] + both
            dn_all = dot(w_low[g], dm_all[g, :, wide], ((0,), (0,)))
            for b in range(h * size, (h + 1) * size):
                rows = slice(b * span, (b + 1) * span)
                k = b - h * size
                dn = dn_all[:, k * chans : (k + 1) * chans]
                scaled = scaled_i[save, rows, lanes].astype(f32)
                prod = dn * scaled
                acc_g[g] = acc_g[g] + jnp.sum(prod.reshape(-1, 8, chans), axis=0)
                acc_s[g] = acc_s[g] + jnp.sum(dn.reshape(-1, 8, chans), axis=0)
                e = dn * gain[first + g]
                mean_e = jnp.mean(e, axis=1, keepdims=True)
                mean_s = jnp.mean(prod * gain[first + g], axis=1, keepdims=True)
                gv[rows, lanes] = (
                    w1[save, rows, lanes].astype(f32) * (e - mean_e - scaled * mean_s)
                ).astype(bf16)
    lines, mats = [], []
    for g in range(per):
        mats.append(acc[g][:, :span])
        lines.append(jnp.transpose(acc[g][:, span:])[:1])
        lines.append(jnp.sum(acc_g[g], axis=0, keepdims=True))
        lines.append(jnp.sum(acc_s[g], axis=0, keepdims=True))
    even, odd = mats
    diag = jnp.sum(jnp.where(row == col, odd, 0.0), axis=0, keepdims=True)
    square = jnp.where(row >= col, even, jnp.transpose(odd))
    pad = jnp.zeros((LINES - 7, span), f32)
    lines = jnp.concatenate(lines + [diag, pad], axis=0)
    encode(small, here, square, lines)


def backward(sc, rel, index, d_out, w, saves, w_mix, gain, shift, carried):
    num_dp = lax.axis_size("dp")
    length, depth = d_out.shape
    groups, span, _ = w_mix.shape
    rows = w.shape[0]
    width = rows * num_dp
    chans = width // groups
    per = 2
    chunk = per * chans
    steps = rows // chunk

    def at(j, sc):
        return jnp.bitwise_xor(rel, sc[0]) * steps + j

    whole = pl.BlockSpec(memory_space=pltpu.VMEM)
    in_specs = [whole] * 9
    args = [d_out, w.reshape(steps, chunk, depth), *saves, w_mix, gain, shift]
    aliases = {}
    if carried is not None:
        for k, value in enumerate(carried):
            aliases[1 + len(args)] = k
            in_specs.append(pl.BlockSpec(memory_space=pl.ANY))
            args.append(value)
    out = pl.BlockSpec((length, chunk), lambda j, sc: (0, at(j, sc)))
    shape = jax.ShapeDtypeStruct((length, width), bf16)
    return pl.pallas_call(
        functools.partial(backward_kernel, (span, chans, per, index * steps, at)),
        grid_spec=pltpu.PrefetchScalarGridSpec(
            num_scalar_prefetch=1,
            grid=(steps,),
            in_specs=in_specs,
            out_specs=[
                out,
                out,
                whole,
            ],
            scratch_shapes=[
                pltpu.VMEM((length, chunk), bf16),
                pltpu.VMEM((per, span, length // span * chans), bf16),
                pltpu.VMEM((per, 2 * span, length // span * chans), bf16),
            ],
        ),
        out_shape=[
            shape,
            shape,
            jax.ShapeDtypeStruct((steps, span + 2 * LINES, span), bf16),
        ],
        input_output_aliases=aliases,
        cost_estimate=pl.CostEstimate(
            flops=2 * length * rows * depth, transcendentals=0, bytes_accessed=0
        ),
        compiler_params=pltpu.CompilerParams(vmem_limit_bytes=VMEM),
    )(sc, *args)


def add(a, b):
    return (a.astype(f32) + b.astype(f32)).astype(bf16)


def split_kernel(k1, r1, k2, r2, send1, keep1, send2, keep2):
    for k, r, send, keep in ((k1, r1, send1, keep1), (k2, r2, send2, keep2)):
        for i in range(k.shape[0]):
            for j in range(k.shape[1]):
                send[i, j] = add(k[i, j, 1], r[i, j, 1])
                keep[i, j] = add(k[i, j, 0], r[i, j, 0])


def join_kernel(k, r, out):
    out[...] = add(k[...], r[...])


def join_more_kernel(k, r, more, out):
    total = k[...].astype(f32) + r[...].astype(f32)
    out[...] = (total + more[...].astype(f32)).astype(bf16)


def merge_kernel(mine, got, out):
    for i in range(mine.shape[0]):
        square, lines = decode(mine, i)
        more, extra = decode(got, i)
        encode(out, i, square + more, lines + extra)


def unpack_kernel(sc, *refs):
    *blocks, grad_w, bias, gain, shift = refs
    steps = blocks[0].shape[0]
    span = blocks[0].shape[2]
    row = lax.broadcasted_iota(jnp.int32, (span, span), 0)
    col = lax.broadcasted_iota(jnp.int32, (span, span), 1)
    for rel, block in enumerate(blocks):
        base = jnp.bitwise_xor(rel, sc[0]) * (2 * steps)
        for j in range(steps):
            square, lines = decode(block, j)
            even = jnp.where(row >= col, square, 0.0)
            odd = jnp.where(row > col, jnp.transpose(square), 0.0)
            odd = jnp.where(row == col, jnp.broadcast_to(lines[6:7], (span, span)), odd)
            for g, value in enumerate((even, odd)):
                at = base + 2 * j + g
                grad_w[at] = value
                for k, ref in enumerate((bias, gain, shift)):
                    ref[pl.ds(at, 1), :] = lines[3 * g + k : 3 * g + k + 1]


def unpack(sc, blocks, groups):
    span = blocks[0].shape[2]
    whole = pl.BlockSpec(memory_space=pltpu.VMEM)
    line = jax.ShapeDtypeStruct((groups, span), f32)
    return pl.pallas_call(
        unpack_kernel,
        in_specs=[pl.BlockSpec(memory_space=pltpu.SMEM)] + [whole] * len(blocks),
        out_specs=[whole] * 4,
        out_shape=[jax.ShapeDtypeStruct((groups, span, span), f32), line, line, line],
        compiler_params=pltpu.CompilerParams(vmem_limit_bytes=VMEM),
        name="unpack",
    )(sc, *blocks)


def flip_kernel(step, value, got, out):
    for j in range(value.shape[0]):
        out[j] = add(value[j], got[j ^ step])


def local(body, shapes, *args):
    return pl.pallas_call(
        body,
        out_shape=[jax.ShapeDtypeStruct(shape, bf16) for shape in shapes],
        in_specs=[pl.BlockSpec(memory_space=pltpu.VMEM)] * len(args),
        out_specs=[pl.BlockSpec(memory_space=pltpu.VMEM)] * len(shapes),
        compiler_params=pltpu.CompilerParams(vmem_limit_bytes=VMEM),
    )(*args)


def assemble_kernel(base, sc, *refs):
    *parts, out = refs
    rest, piece, _ = parts[0].shape
    if base == 0:
        for low in range(4):
            for high in range(rest):
                at = jnp.bitwise_xor(4 * high + low, sc[1]) * piece
                out[pl.ds(pl.multiple_of(at, piece), piece), :] = parts[low][high].astype(f32)
    else:
        out[...] = parts[0][pl.program_id(0)].astype(f32)


def assemble(sc, side, base, parts, carried):
    rest, piece, half = parts[0].shape
    in_specs = [pl.BlockSpec(memory_space=pltpu.VMEM)] * len(parts)
    args, aliases = list(parts), {}
    if carried is not None:
        aliases = {1 + len(args): 0}
        in_specs.append(pl.BlockSpec(memory_space=pl.ANY))
        args.append(carried)

    def body(sc, *refs):
        assemble_kernel(base, sc, *refs[: len(parts)], refs[-1])

    if base == 0:
        out = pl.BlockSpec((rest * 4 * piece, half), lambda p, sc: (0, side))
    else:
        out = pl.BlockSpec((piece, half), lambda p, sc: (jnp.bitwise_xor(4 * p + base, sc[1]), side))
    return pl.pallas_call(
        body,
        grid_spec=pltpu.PrefetchScalarGridSpec(
            num_scalar_prefetch=1,
            grid=(1 if base == 0 else rest,),
            in_specs=in_specs,
            out_specs=out,
        ),
        out_shape=jax.ShapeDtypeStruct((rest * 4 * piece, 2 * half), f32),
        input_output_aliases=aliases,
        compiler_params=pltpu.CompilerParams(vmem_limit_bytes=VMEM),
    )(sc, *args)


def bits_of(count):
    return [1 << k for k in range(count.bit_length() - 1)]


def reduce_small(packed):
    sp_bits, dp_bits = bits_of(lax.axis_size("sp")), bits_of(lax.axis_size("dp"))
    for bit in [dp_bits[0]] + list(reversed(dp_bits[1:])):
        for rel in [r for r in packed if r & bit]:
            got = swap(packed.pop(rel), 0, bit)
            mine = packed[rel ^ bit]
            packed[rel ^ bit] = local(merge_kernel, [mine.shape], mine, got)[0]
    value = packed[0]
    for bit in sp_bits:
        got = swap(value, bit, 0)
        value = local(merge_kernel, [value.shape], value, got)[0]
    blocks = {0: value}
    for bit in dp_bits[1:] + [dp_bits[0]]:
        for rel in list(blocks):
            blocks[rel | bit] = swap(blocks[rel], 0, bit)
    return [blocks[rel] for rel in range(len(blocks))]


def program(u_pre, v_pre, d_out, w_mix, mix_bias, norm_gain, norm_shift, w_out):
    num_sp, num_dp = lax.axis_size("sp"), lax.axis_size("dp")
    shape = u_pre.shape
    width = shape[2]
    groups, _, _ = w_mix.shape
    u, v = u_pre.reshape(-1, width), v_pre.reshape(-1, width)
    d = d_out.reshape(-1, d_out.shape[2])
    sc = jnp.stack([lax.axis_index("dp"), lax.axis_index("sp")]).astype(jnp.int32)
    bias, gain, shift = (a[:, None, :] for a in (mix_bias, norm_gain, norm_shift))
    small = (w_mix, bias, gain, shift)
    u_far, v_far, *small_far = (
        pltpu.with_memory_space_constraint(a, pltpu.HBM) for a in (u, v, *small)
    )

    sp_bits, dp_bits = bits_of(num_sp), bits_of(num_dp)
    bit_a, bit_b, others = sp_bits[0], sp_bits[1], sp_bits[2:]
    piece = width // num_dp // num_sp
    depth = d.shape[1]
    half = depth // 2
    rest = num_sp // 4
    count = num_dp // 4
    weights = {0: w_out, 1: swap(w_out, 0, 1)}
    for rel in range(2, num_dp, 2):
        top = 1 << (rel.bit_length() - 1)
        weights[rel] = swap(weights[rel - top], 0, top)
    for rel in range(2, num_dp, 2):
        weights[rel + 1] = swap(weights[rel], 0, 1)

    saves, heads = {}, {}

    def front(rel, recv):
        if rel == num_dp - 1:
            out = forward(sc, rel, count, False, u_far, v_far, d, *small_far, recv)
        else:
            out = forward(sc, rel, count, True, u, v, d, *small, recv)
        kept = out[-4:]
        for i in range(count):
            saves[rel - 2 * i] = (kept, i)
        heads[rel] = out[:-4]

    packed = {}

    def back(rel, carried):
        kept, i = saves[rel]
        *carried, packed[rel] = backward(
            sc, rel, i, d, weights[rel], kept, w_mix, gain, shift, carried
        )
        return carried

    top, low = num_dp - 1, num_dp // 2 - 1
    front(top, None)
    recv_a = swap(heads[top][0], 0, 1)
    front(low, None)
    recv_b = swap(heads[low][0], 0, 1)
    front(top - 1, recv_a)
    s1a, k1a, s2a, k2a = heads[top - 1]
    r1a, r2a = swap(s1a, bit_a, 0), swap(s2a, bit_b, 0)
    front(low - 1, recv_b)
    s1b, k1b, s2b, k2b = heads[low - 1]
    r1b, r2b = swap(s1b, bit_a, 0), swap(s2b, bit_b, 0)
    shaped = (count, rest, 2, piece, half)
    done = (count, rest, piece, half)

    def split(*arrays):
        return local(split_kernel, [done] * 4, *(x.reshape(shaped) for x in arrays))

    carried = back(1, None)
    t1a, k1a, t2a, k2a = split(k1a, r1a, k2a, r2a)
    r1a, r2a = swap(t1a, bit_b, 0), swap(t2a, bit_a, 0)
    carried = back(0, carried)
    t1b, k1b, t2b, k2b = split(k1b, r1b, k2b, r2b)
    r1b, r2b = swap(t1b, bit_b, 0), swap(t2b, bit_a, 0)
    ends_a, ends_b = ((k1a, r1a), (k2a, r2a)), ((k1b, r1b), (k2b, r2b))
    chip = []
    for pair in ends_a:
        send = local(join_kernel, [done], *pair)[0]
        chip.append(swap(send, 0, dp_bits[-1]))
    carried = back(2, carried)
    sides = [local(join_more_kernel, [done], *pair, x)[0] for pair, x in zip(ends_b, chip)]
    for bit in reversed(dp_bits[1:-1]):
        middle = sides[0].shape[0] // 2
        sides = [add(x[middle:], swap(x[:middle], 0, bit)) for x in sides]
    sides = [x[0] for x in sides]
    for k, bit in enumerate(others):
        got = [swap(x, bit, 0) for x in sides]
        if k == len(others) - 1:
            for rel in range(3, num_dp):
                carried = back(rel, carried)
        flip = functools.partial(flip_kernel, 1 << k)
        sides = [local(flip, [x.shape], x, y)[0] for x, y in zip(sides, got)]
    grad_u, grad_v = carried
    pieces = []
    for x, near, far in zip(sides, (bit_a, bit_b), (bit_b, bit_a)):
        one, two = swap(x, near, 0), swap(x, far, 0)
        three = swap(one, far, 0)
        middle = (one, two) if near == bit_a else (two, one)
        pieces.append([x, *middle, three])
    grad_w_out = None
    for side in (1, 0):
        x, one, two, three = pieces[side]
        grad_w_out = assemble(sc, side, 0, [x, one, two, x], grad_w_out)
    for side in (1, 0):
        grad_w_out = assemble(sc, side, 3, [pieces[side][3]], grad_w_out)
    sums = reduce_small(packed)
    grads = unpack(sc, sums, groups)
    return (grad_u.reshape(shape), grad_v.reshape(shape), grad_w_out, *grads)


def solution(mesh):
    return jax.shard_map(
        program,
        mesh=mesh,
        in_specs=(
            P("dp", "sp", None),
            P("dp", "sp", None),
            P("dp", "sp", None),
            P(),
            P(),
            P(),
            P(),
            P("dp", None),
        ),
        out_specs=(P("dp", "sp", None), P("dp", "sp", None), P("dp", None), P(), P(), P(), P()),
        check_vma=False,
    )
```
